32 devices in a mesh: kv: 16 (over z, y, x), tp: 2 (over core).
Axes of the slice: x: 2, y: 2, z: 4, core: 2. Of those that a mesh axis runs over, the one named last changes fastest.
Arguments:
- tokens: bfloat16 [64, 4096], P(None, 'kv')
- lengths: int32 [16], replicated, may hold values from 1 to 4, 28 in all
- memory: float32 [16, 16, 128, 128], P('kv', 'tp'), may hold values from -0.6 to 0.6
- norm_gain: float32 [4096], P('kv'), may hold values from 0.1 to 1.9
- w_query: bfloat16 [4096, 2048], P('kv', 'tp'), may hold values from -0.09375 to 0.09375
- w_key: bfloat16 [4096, 2048], P('kv', 'tp'), may hold values from -0.09375 to 0.09375
- w_value: bfloat16 [4096, 2048], P('kv', 'tp'), may hold values from -0.09375 to 0.09375
- w_outgate: bfloat16 [4096, 2048], P('kv', 'tp'), may hold values from -0.09375 to 0.09375
- w_alpha: bfloat16 [4096, 16], P('kv'), may hold values from -0.09375 to 0.09375
- w_beta: bfloat16 [4096, 16], P('kv'), may hold values from -0.09375 to 0.09375
- decay_log: float32 [16], P('tp'), may hold values from -4 to 0.5
- decay_bias: float32 [16], P('tp'), may hold values from -1 to 1
- head_gain: float32 [128], replicated, may hold values from 0.1 to 1.9
- w_output: bfloat16 [2048, 4096], P('tp', 'kv'), may hold values from -0.125 to 0.125
- mlp_gain: float32 [4096], P('kv'), may hold values from 0.1 to 1.9
- w_gate: bfloat16 [4096, 11264], P('kv', 'tp'), may hold values from -0.09375 to 0.09375
- w_up: bfloat16 [4096, 11264], P('kv', 'tp'), may hold values from -0.09375 to 0.09375
- w_down: bfloat16 [11264, 4096], P('tp', 'kv'), may hold values from -0.0546875 to 0.0546875
Outputs:
- layer_out: bfloat16 [64, 4096], P(None, 'kv')
- new_memory: float32 [16, 16, 128, 128], P('kv', 'tp')
The draws below stay inside these ranges and needn't reach their ends.
Inputs may be any that keep to these rules, and one draw needn't show every extreme that they name: How many of a sequence's 4 slots hold live tokens; the live ones come first; the lengths add up to seven quarters of 16, rounded down.
All inputs are finite; a program needn't handle non-finite values.
Results may differ from the reference program's by a relative error of at most 0.012.
Values may be sent and summed in bfloat16 or wider, within the bound.
A program may use at most 64 MiB of HBM per device.

```python
import math
import jax
import jax.numpy as jnp
import numpy as np
from jax import lax

D = 4096
H = 16
DK = 128
DV = 128
FF = 11264
NEW = 4
SEQS = 16


def draw_tokens(key, part):
    first, second, third = jax.random.split(key, 3)
    total_rows = SEQS * NEW
    column_ramp = jnp.exp(jnp.linspace(math.log(0.5), math.log(2.0), D))
    column_noise = jnp.exp(jax.random.uniform(second, (D,), jnp.float32, math.log(0.7), math.log(1.4)))
    row_scale = jnp.exp(jax.random.uniform(third, (total_rows, 1), jnp.float32, math.log(0.3), math.log(3.0)))
    base = jax.random.normal(first, (total_rows, D), jnp.float32)
    return (base * column_ramp * column_noise * row_scale).astype(jnp.bfloat16)


def level_of(key, extent, pieces, least, largest):
    level = 1.0
    for position, parts in pieces:
        draws = jax.random.uniform(jax.random.fold_in(jax.random.fold_in(key, 6), position), (parts,), jnp.float32, least / len(pieces), largest / len(pieces))
        level = level * jnp.repeat(jnp.exp(draws), extent[position] // parts).reshape((-1,) + (1,) * (len(extent) - 1 - position))
    return level


def length_profile(count, total, reach, slope):
    weights = [(1 << 20) // math.isqrt(rank ** slope) + 1 for rank in range(2, count + 1)]
    surplus, counts = total - reach - (count - 1), [1] * (count - 1)
    while surplus > 0:
        movable = [i for i in range(count - 1) if counts[i] < reach]
        whole, budget = sum([weights[i] for i in movable]), surplus
        for i in movable:
            more = min(reach - counts[i], max(1, budget * weights[i] // whole), surplus)
            counts[i] = counts[i] + more
            surplus = surplus - more
    return np.array([reach] + counts)


def ragged(stream_key, count, total, bound, slope):
    if count == 2:
        one = jax.random.randint(stream_key, (), max(1, total - bound), min(bound, total - 1) + 1)
        return jnp.stack([one, total - one])
    sizes = jnp.asarray(length_profile(count, total, bound, slope), jnp.int32)
    pairs = (count - 1) // 2
    giver, sink = sizes[1:1 + 2 * pairs:2], sizes[2:2 + 2 * pairs:2]
    room = jnp.minimum(giver - 1, bound - sink)
    passed = jax.random.randint(jax.random.fold_in(stream_key, 1), (pairs,), 0, 1 << 20) % (room + 1)
    sizes = sizes.at[1:1 + 2 * pairs:2].set(giver - passed).at[2:2 + 2 * pairs:2].set(sink + passed)
    return sizes[jax.random.permutation(jax.random.fold_in(stream_key, 2), count)]


def centred(rng, extent, spread, bound, cuts=(), held_as=jnp.bfloat16):
    gain = level_of(rng, extent, cuts, -0.22, 0.18) if cuts else 1.0
    values = jax.random.normal(rng, extent, jnp.float32) * spread * gain
    return jnp.minimum(jnp.maximum(values, -bound), bound).astype(held_as)


def setup_inputs(seed: int = 0) -> dict:
    streams_of = jax.random.split(jax.random.key(seed), 19)
    return {
        "tokens": draw_tokens(jax.random.fold_in(streams_of[18], 71), 0),
        "lengths": ragged(streams_of[1], SEQS, SEQS * 7 // 4, NEW, 2).astype(jnp.int32),
        "memory": centred(streams_of[2], (SEQS, H, DK, DV), 0.1, 0.6, ((0, 16), (1, 2)), jnp.float32),
        "norm_gain": jnp.clip(1.0 + 0.18 * jax.random.normal(streams_of[3], (D,), jnp.float32), 0.1, 1.9),
        "w_query": centred(streams_of[4], (D, H * DK), D ** -0.5, 0.09375, ((0, 16), (1, 2))),
        "w_key": centred(streams_of[5], (D, H * DK), D ** -0.5, 0.09375, ((0, 16), (1, 2))),
        "w_value": centred(streams_of[6], (D, H * DV), D ** -0.5, 0.09375, ((0, 16), (1, 2))),
        "w_outgate": centred(streams_of[7], (D, H * DV), D ** -0.5, 0.09375, ((0, 16), (1, 2))),
        "w_alpha": centred(streams_of[8], (D, H), D ** -0.5, 0.09375, ((0, 16),)),
        "w_beta": centred(streams_of[9], (D, H), D ** -0.5, 0.09375, ((0, 16),)),
        "decay_log": jnp.clip(-4.0 + 4.5 * jax.random.uniform(streams_of[10], (H,), jnp.float32) ** level_of(streams_of[10], (H,), ((0, 2),), -0.2, 0.2), -4.0, 0.5),
        "decay_bias": jnp.clip(jax.random.uniform(streams_of[11], (H,), jnp.float32, -1.0, 1.0) * level_of(streams_of[11], (H,), ((0, 2),), -0.4, 0.0), -1.0, 1.0),
        "head_gain": jnp.clip(1.0 + 0.18 * jax.random.normal(streams_of[12], (DV,), jnp.float32), 0.1, 1.9),
        "w_output": centred(streams_of[13], (H * DV, D), (H * DV) ** -0.5, 0.125, ((0, 2), (1, 16))),
        "mlp_gain": jnp.clip(1.0 + 0.18 * jax.random.normal(streams_of[14], (D,), jnp.float32), 0.1, 1.9),
        "w_gate": centred(streams_of[15], (D, FF), D ** -0.5, 0.09375, ((0, 16), (1, 2))),
        "w_up": centred(streams_of[16], (D, FF), D ** -0.5, 0.09375, ((0, 16), (1, 2))),
        "w_down": centred(streams_of[17], (FF, D), FF ** -0.5, 0.0546875, ((0, 2), (1, 16))),
    }


epsilon = 1e-06

def unit_rows(values):
    return values * lax.rsqrt(lax.optimization_barrier(jnp.sum(values * values, axis=-1, keepdims=True)) + epsilon)

def advance(memory, queries, key_rows, value_rows, decays, betas):
    outputs = []
    for step in range(queries.shape[1]):
        memory = jnp.exp(decays[:, step])[:, :, None, None] * memory
        predicted = jnp.einsum('shde,shd->she', memory, key_rows[:, step], precision=lax.Precision.HIGHEST)
        correction = betas[:, step][:, :, None] * (value_rows[:, step] - predicted)
        memory = memory + key_rows[:, step][:, :, :, None] * correction[:, :, None, :]
        outputs.append(jnp.einsum('shde,shd->she', memory, queries[:, step], precision=lax.Precision.HIGHEST))
    return (memory, jnp.stack(outputs, axis=1))

def reference(tokens, lengths, memory, norm_gain, w_query, w_key, w_value, w_outgate, w_alpha, w_beta, decay_log, decay_bias, head_gain, w_output, mlp_gain, w_gate, w_up, w_down):
    total_rows = tokens.shape[0]
    token_f = tokens.astype(jnp.float32)
    rstd = lax.rsqrt(lax.optimization_barrier(jnp.mean(token_f * token_f, axis=1, keepdims=True)) + epsilon)
    scaled = (token_f * norm_gain).astype(jnp.bfloat16)

    def project(weight):
        return jnp.dot(scaled, weight, preferred_element_type=jnp.float32) * rstd
    queries = project(w_query).astype(jnp.bfloat16)
    key_rows = project(w_key).astype(jnp.bfloat16)
    value_rows = project(w_value).astype(jnp.bfloat16)
    outgate = project(w_outgate).astype(jnp.bfloat16)
    alphas = project(w_alpha)
    beta_pre = project(w_beta)
    live = jnp.arange(NEW, dtype=jnp.int32)[None, :] < lengths[:, None]
    query_h = unit_rows(queries.astype(jnp.float32).reshape(SEQS, NEW, H, DK)) * DK ** (-0.5)
    key_h = unit_rows(key_rows.astype(jnp.float32).reshape(SEQS, NEW, H, DK))
    value_h = value_rows.astype(jnp.float32).reshape(SEQS, NEW, H, DV)
    decays = -jnp.exp(decay_log) * jax.nn.softplus(alphas + decay_bias)
    decays = jnp.where(live[:, :, None], decays.reshape(SEQS, NEW, H), 0.0)
    betas = jnp.where(live[:, :, None], jax.nn.sigmoid(beta_pre).reshape(SEQS, NEW, H), 0.0)
    new_memory, attended = advance(memory, query_h, key_h, value_h, decays, betas)
    attended = attended * lax.rsqrt(lax.optimization_barrier(jnp.mean(attended * attended, axis=-1, keepdims=True)) + epsilon)
    gate_h = outgate.astype(jnp.float32).reshape(SEQS, NEW, H, DV)
    mixed = (attended * head_gain * jax.nn.silu(gate_h)).astype(jnp.bfloat16).reshape(total_rows, H * DV)
    hidden = (token_f + jnp.dot(mixed, w_output, preferred_element_type=jnp.float32)).astype(jnp.bfloat16)
    hidden_f = hidden.astype(jnp.float32)
    rstd2 = lax.rsqrt(lax.optimization_barrier(jnp.mean(hidden_f * hidden_f, axis=1, keepdims=True)) + epsilon)
    hscaled = (hidden_f * mlp_gain).astype(jnp.bfloat16)
    gate_rows = jnp.dot(hscaled, w_gate, preferred_element_type=jnp.float32) * rstd2
    up_rows = jnp.dot(hscaled, w_up, preferred_element_type=jnp.float32) * rstd2
    active = (jax.nn.silu(gate_rows) * up_rows).astype(jnp.bfloat16)
    result = hidden_f + jnp.dot(active, w_down, preferred_element_type=jnp.float32)
    layer_out = jnp.where(live.reshape(total_rows)[:, None], result, 0.0).astype(jnp.bfloat16)
    return (layer_out, new_memory)
```

```python
import jax
import jax.numpy as jnp
from jax import lax
from jax.experimental import pallas as pl
from jax.experimental.pallas import tpu as pltpu
from jax.sharding import PartitionSpec as P

D = 4096
DK = 128
DV = 128
NEW = 4


epsilon = 1e-06


def unit_rows(values):
    return values * lax.rsqrt(jnp.sum(values * values, axis=-1, keepdims=True) + epsilon)


def advance(memory, queries, key_rows, value_rows, decays, betas):
    outputs = []
    for step in range(queries.shape[1]):
        memory = jnp.exp(decays[:, step])[:, :, None, None] * memory
        predicted = jnp.einsum(
            "shde,shd->she", memory, key_rows[:, step], precision=lax.Precision.HIGHEST
        )
        correction = betas[:, step][:, :, None] * (value_rows[:, step] - predicted)
        memory = memory + key_rows[:, step][:, :, :, None] * correction[:, :, None, :]
        outputs.append(
            jnp.einsum("shde,shd->she", memory, queries[:, step], precision=lax.Precision.HIGHEST)
        )
    return (memory, jnp.stack(outputs, axis=1))


def per_device(
    tokens,
    lengths,
    memory,
    norm_gain,
    w_query,
    w_key,
    w_value,
    w_outgate,
    w_alpha,
    w_beta,
    decay_log,
    decay_bias,
    head_gain,
    w_output,
    mlp_gain,
    w_gate,
    w_up,
    w_down,
):
    total_rows = tokens.shape[0]
    kv_count = lax.axis_size("kv")
    kv_place = lax.axis_index("kv")
    tp_place = lax.axis_index("tp")
    own_rows = total_rows // kv_count
    seq_dev = memory.shape[0]
    heads_dev = memory.shape[1]
    token_f = tokens.astype(jnp.float32)
    squares = jnp.sum(token_f * token_f, axis=1)
    scaled = (token_f * norm_gain).astype(jnp.bfloat16)
    part_query = jnp.dot(scaled, w_query, preferred_element_type=jnp.float32)
    part_key = jnp.dot(scaled, w_key, preferred_element_type=jnp.float32)
    part_value = jnp.dot(scaled, w_value, preferred_element_type=jnp.float32)
    part_gate = jnp.dot(scaled, w_outgate, preferred_element_type=jnp.float32)
    part_alpha = jnp.dot(scaled, w_alpha, preferred_element_type=jnp.float32)
    part_beta = jnp.dot(scaled, w_beta, preferred_element_type=jnp.float32)
    all_squares = lax.psum(squares, "kv")
    sum_query, sum_key, sum_value, sum_gate, sum_alpha, sum_beta = (
        lax.psum_scatter(part_query, "kv", scatter_dimension=0, tiled=True),
        lax.psum_scatter(part_key, "kv", scatter_dimension=0, tiled=True),
        lax.psum_scatter(part_value, "kv", scatter_dimension=0, tiled=True),
        lax.psum_scatter(part_gate, "kv", scatter_dimension=0, tiled=True),
        lax.psum_scatter(part_alpha, "kv", scatter_dimension=0, tiled=True),
        lax.psum_scatter(part_beta, "kv", scatter_dimension=0, tiled=True),
    )
    own_squares = lax.dynamic_slice_in_dim(all_squares, kv_place * own_rows, own_rows)
    rstd = lax.rsqrt(own_squares / D + epsilon)[:, None]
    queries = (sum_query * rstd).astype(jnp.bfloat16)
    key_rows = (sum_key * rstd).astype(jnp.bfloat16)
    value_rows = (sum_value * rstd).astype(jnp.bfloat16)
    outgate = (sum_gate * rstd).astype(jnp.bfloat16)
    alphas = lax.dynamic_slice_in_dim(sum_alpha * rstd, tp_place * heads_dev, heads_dev, 1)
    beta_pre = lax.dynamic_slice_in_dim(sum_beta * rstd, tp_place * heads_dev, heads_dev, 1)
    own_lengths = lax.dynamic_slice_in_dim(lengths, kv_place * seq_dev, seq_dev)
    live = jnp.arange(NEW, dtype=jnp.int32)[None, :] < own_lengths[:, None]
    query_h = unit_rows(queries.astype(jnp.float32).reshape(seq_dev, NEW, heads_dev, DK)) * DK ** (
        -0.5
    )
    key_h = unit_rows(key_rows.astype(jnp.float32).reshape(seq_dev, NEW, heads_dev, DK))
    value_h = value_rows.astype(jnp.float32).reshape(seq_dev, NEW, heads_dev, DV)
    decays = -jnp.exp(decay_log) * jax.nn.softplus(alphas + decay_bias)
    decays = jnp.where(live[:, :, None], decays.reshape(seq_dev, NEW, heads_dev), 0.0)
    betas = jnp.where(
        live[:, :, None], jax.nn.sigmoid(beta_pre).reshape(seq_dev, NEW, heads_dev), 0.0
    )
    new_memory, attended = advance(memory, query_h, key_h, value_h, decays, betas)
    attended = attended * lax.rsqrt(jnp.mean(attended * attended, axis=-1, keepdims=True) + epsilon)
    gate_h = outgate.astype(jnp.float32).reshape(seq_dev, NEW, heads_dev, DV)
    mixed = (
        (attended * head_gain * jax.nn.silu(gate_h))
        .astype(jnp.bfloat16)
        .reshape(own_rows, heads_dev * DV)
    )
    attn_terms = jnp.dot(
        lax.all_gather(mixed, "kv", axis=0, tiled=True),
        w_output,
        preferred_element_type=jnp.float32,
    )
    attn_total = lax.psum(attn_terms, "tp")
    hidden = (token_f + attn_total).astype(jnp.bfloat16)
    hidden_f = hidden.astype(jnp.float32)
    hidden_squares = jnp.sum(hidden_f * hidden_f, axis=1)
    hscaled = (hidden_f * mlp_gain).astype(jnp.bfloat16)
    all_live = (jnp.arange(NEW, dtype=jnp.int32)[None, :] < lengths[:, None]).reshape(total_rows)
    part_gate_rows = jnp.dot(hscaled, w_gate, preferred_element_type=jnp.float32)
    part_up_rows = jnp.dot(hscaled, w_up, preferred_element_type=jnp.float32)
    gate_rows, up_rows, mlp_squares = lax.psum((part_gate_rows, part_up_rows, hidden_squares), "kv")
    rstd2 = lax.rsqrt(mlp_squares / D + epsilon)[:, None]
    active = (jax.nn.silu(gate_rows * rstd2) * (up_rows * rstd2)).astype(jnp.bfloat16)
    feed_terms = jnp.dot(active, w_down, preferred_element_type=jnp.float32)
    feed_total = lax.psum(feed_terms.astype(jnp.bfloat16), "tp").astype(jnp.float32)
    layer_out = jnp.where(all_live[:, None], hidden_f + feed_total, 0.0).astype(jnp.bfloat16)
    return (layer_out, new_memory)


F32 = jnp.float32
BF16 = jnp.bfloat16
HIGH = lax.Precision.HIGHEST
TILE = 128
GROUP = 8


def iota(shape, axis):
    return lax.broadcasted_iota(jnp.int32, shape, axis)


def dot(a, b, precision=None):
    return jnp.dot(a, b, preferred_element_type=F32, precision=precision)


def fused(
    lens,
    tokens,
    norm_gain,
    decay_log,
    decay_bias,
    head_gain,
    mlp_gain,
    w_alpha,
    w_beta,
    memory,
    w_query,
    w_key,
    w_value,
    w_outgate,
    w_output,
    w_gate,
    w_up,
    w_down,
    out,
    new_memory,
    v_mem,
    v_query,
    v_key,
    v_value,
    v_outgate,
    v_output,
    v_gate,
    v_up,
    v_down,
    proj_send,
    proj_recv,
    rs_buf,
    xs_buf,
    kq_buf,
    r_buf,
    u_buf,
    a_buf,
    ab_buf,
    mix_buf,
    mix_all,
    tp_send,
    tp_recv,
    sq_send,
    sq_recv,
    gu_send,
    gu_recv,
    act_all,
    load_sem,
    send_sem,
    recv_sem,
    tp_sem,
):
    kv_count = mix_all.shape[0]
    me = lax.axis_index("kv")
    tp = lax.axis_index("tp")
    rows, width = tokens.shape
    heads = v_mem.shape[0]
    wide = heads * DV
    compact = tp_send.shape[1]
    groups = compact // GROUP
    zones = kv_count // groups
    chunk = gu_send.shape[2]
    total_width = width * kv_count

    barrier = pltpu.get_barrier_semaphore()

    @pl.loop(1, kv_count)
    def _(off):
        pl.semaphore_signal(
            barrier,
            inc=1,
            device_id={"kv": lax.rem(me + off, kv_count)},
            device_id_type=pl.DeviceIdType.MESH,
        )

    pl.semaphore_signal(
        barrier, inc=1, device_id={"tp": 1 - tp}, device_id_type=pl.DeviceIdType.MESH
    )
    pairs = [
        (w_query, v_query),
        (w_key, v_key),
        (w_value, v_value),
        (w_outgate, v_outgate),
        (memory, v_mem),
        (w_output, v_output),
        (w_gate, v_gate),
        (w_up, v_up),
        (w_down, v_down),
    ]
    loads = [pltpu.make_async_copy(a, b, load_sem.at[n]) for n, (a, b) in enumerate(pairs)]
    for load in loads:
        load.start()

    def remote(src, dst, phase, slot, partner, arrival):
        return pltpu.make_async_remote_copy(
            src_ref=src,
            dst_ref=dst,
            send_sem=send_sem.at[phase, slot],
            recv_sem=recv_sem.at[phase, arrival],
            device_id={"kv": partner},
            device_id_type=pl.DeviceIdType.MESH,
        )

    def tp_swap(phase, value):
        tp_send[phase] = value
        swap = pltpu.make_async_remote_copy(
            src_ref=tp_send.at[phase],
            dst_ref=tp_recv.at[phase],
            send_sem=tp_sem.at[phase, 0],
            recv_sem=tp_sem.at[phase, 1],
            device_id={"tp": 1 - tp},
            device_id_type=pl.DeviceIdType.MESH,
        )
        swap.start()
        swap.wait()
        return value + tp_recv[phase]

    all_rows = kv_count * 4 * NEW
    row = iota((all_rows, rows), 0)
    spread = jnp.where(
        iota((all_rows, rows), 1) == (row >> 4) * NEW + (row & 3), 1.0, 0.0
    ).astype(BF16)
    tok = tokens[...]
    scaled = (tok.astype(F32) * norm_gain[...]).astype(BF16)
    wide_tok = dot(spread, tok)
    wide_scaled = dot(spread, scaled)
    squares = jnp.sum(wide_tok * wide_tok, axis=1, keepdims=True)
    part_of = (iota((all_rows, width), 0) >> 2) & 3
    all_heads = w_alpha.shape[1]
    place = iota((all_heads, TILE), 1)
    head_of = iota((all_heads, TILE), 0)
    w_small = dot(w_alpha[...], jnp.where(place == head_of, 1.0, 0.0).astype(BF16)) + dot(
        w_beta[...], jnp.where(place == head_of + all_heads, 1.0, 0.0).astype(BF16)
    )
    small = dot(wide_scaled.astype(BF16), w_small.astype(BF16))
    lane = iota((all_rows, TILE), 1)
    small = jnp.where(lane == 2 * all_heads, squares, small)
    part_small = (iota((all_rows, TILE), 0) >> 2) & 3
    first = small.astype(BF16).astype(F32)
    second = (small - first).astype(BF16).astype(F32)
    third = small - first - second
    pieces = jnp.where(
        part_small == 0,
        first,
        jnp.where(part_small == 1, second, jnp.where(part_small == 2, third, 0.0)),
    )
    proj_send[:, :, wide:] = pieces.astype(BF16).reshape(kv_count, 16, TILE)
    masked = [jnp.where(part_of == p, wide_scaled, 0.0).astype(BF16) for p in range(4)]
    for load in loads[:4]:
        load.wait()
    half = wide // 2
    for c in range(2):
        cols = slice(c * half, (c + 1) * half)
        acc = dot(masked[0], v_query[:, cols])
        acc = acc + dot(masked[1], v_key[:, cols])
        acc = acc + dot(masked[2], v_value[:, cols])
        acc = acc + dot(masked[3], v_outgate[:, cols])
        proj_send[:, :, cols] = acc.astype(BF16).reshape(kv_count, 16, half)

    pl.semaphore_wait(barrier, kv_count)

    @pl.loop(1, kv_count)
    def _(off):
        to = lax.rem(me + off, kv_count)
        remote(proj_send.at[to], proj_recv.at[me], 0, to, to, me).start()

    slots_wide = kv_count * heads * NEW
    shape_a = (1, rows)
    shape_b = (1, slots_wide)
    shape_c = (rows, compact)
    length_a = jnp.zeros(shape_a, jnp.int32)
    start_a = jnp.zeros(shape_a, jnp.int32)
    length_b = jnp.zeros(shape_b, jnp.int32)
    start_b = jnp.zeros(shape_b, jnp.int32)
    length_c = jnp.zeros(shape_c, jnp.int32)
    start_c = jnp.zeros(shape_c, jnp.int32)
    seq_a = iota(shape_a, 1) >> 2
    seq_b = iota(shape_b, 1) >> 5
    seq_c = iota(shape_c, 0) >> 2
    begin = jnp.int32(0)
    for s in range(kv_count):
        length_a = jnp.where(seq_a == s, lens[s], length_a)
        start_a = jnp.where(seq_a == s, begin, start_a)
        length_b = jnp.where(seq_b == s, lens[s], length_b)
        start_b = jnp.where(seq_b == s, begin, start_b)
        length_c = jnp.where(seq_c == s, lens[s], length_c)
        start_c = jnp.where(seq_c == s, begin, start_c)
        begin = begin + lens[s]
    slot_a = iota(shape_a, 1) & 3
    rank_a = jnp.where(slot_a < length_a, start_a + slot_a, -1)
    pack = jnp.where(rank_a == iota((compact, rows), 0), 1.0, 0.0).astype(BF16)
    slot_c = iota(shape_c, 0) & 3
    rank_c = jnp.where(slot_c < length_c, start_c + slot_c, -1)
    unpack = jnp.where(rank_c == iota(shape_c, 1), 1.0, 0.0).astype(BF16)
    slot_b = iota(shape_b, 1) & 3
    head_b = (iota(shape_b, 1) >> 2) & (heads - 1)
    rank_b = jnp.where(slot_b < length_b, head_b * compact + start_b + slot_b, -1)
    collect = jnp.where(rank_b == iota((heads * compact, slots_wide), 0), 1.0, 0.0).astype(BF16)
    tok_packed = dot(pack, tok)

    total = proj_send[me].astype(F32)
    for off in range(1, kv_count):
        src = lax.rem(me + off, kv_count)
        remote(proj_send.at[src], proj_recv.at[src], 0, src, src, src).wait_recv()
        total = total + proj_recv[src].astype(F32)
    ab_buf[...] = total[:, wide:]
    small = ab_buf[0:4, :] + ab_buf[4:8, :] + ab_buf[8:12, :]
    lane = iota((NEW, TILE), 1)
    mean_sq = jnp.sum(jnp.where(lane == 2 * all_heads, small, 0.0), axis=1, keepdims=True)
    rstd = lax.rsqrt(mean_sq / total_width + epsilon)
    rstd_wide = jnp.broadcast_to(rstd, (NEW, TILE))
    small = small * rstd
    ab_buf[0:4, :] = small
    for p in range(4):
        rs_buf[p * NEW : (p + 1) * NEW, :] = rstd_wide
    scale = rs_buf[...]
    for h in range(heads):
        piece = total[:, h * DV : (h + 1) * DV] * scale
        xs_buf[h * 16 : (h + 1) * 16, :] = piece.astype(BF16).astype(F32)

    def slot_rows(ref, index, stride):
        return ref[pl.ds(index, heads, stride=stride), :]

    query, key_rows, value, gate = (
        [slot_rows(xs_buf, p * NEW + t, 16) for t in range(NEW)] for p in range(4)
    )
    query = [unit_rows(x) * DK ** (-0.5) for x in query]
    key_rows = [unit_rows(x) for x in key_rows]
    eye = iota((heads, heads), 0) == iota((heads, heads), 1)
    rate = jnp.sum(jnp.where(eye, jnp.exp(decay_log[...]), 0.0), axis=1, keepdims=True)
    bias = jnp.sum(jnp.where(eye, decay_bias[...], 0.0), axis=1, keepdims=True)
    pick = iota((heads, TILE), 1) - iota((heads, TILE), 0)
    own_length = jnp.full((heads, 1), lens[me], jnp.int32)
    decay, beta = [], []
    for t in range(NEW):
        line = ab_buf[t : t + 1, :]
        alpha = jnp.sum(jnp.where(pick == tp * heads, line, 0.0), axis=1, keepdims=True)
        write = jnp.sum(
            jnp.where(pick == tp * heads + all_heads, line, 0.0), axis=1, keepdims=True
        )
        x = alpha + bias
        soft = jnp.maximum(x, 0.0) + jnp.log1p(jnp.exp(-jnp.abs(x)))
        live = own_length > t
        decay.append(jnp.exp(jnp.where(live, -rate * soft, 0.0)))
        beta.append(jnp.where(live, jax.nn.sigmoid(write), 0.0))
    for t in range(NEW):
        kq_buf[pl.ds(t, heads, stride=8), :] = key_rows[t]
        kq_buf[pl.ds(NEW + t, heads, stride=8), :] = query[t]
    loads[4].wait()
    for h in range(heads):
        r_buf[h * 8 : (h + 1) * 8, :] = dot(kq_buf[h * 8 : (h + 1) * 8, :], v_mem[h], HIGH)
    seen_k = [slot_rows(r_buf, t, 8) for t in range(NEW)]
    seen_q = [slot_rows(r_buf, NEW + t, 8) for t in range(NEW)]

    def inner(a, b):
        return jnp.sum(a * b, axis=1, keepdims=True)

    corrections = []
    for t in range(NEW):
        for r in range(t, NEW):
            seen_k[r] = seen_k[r] * decay[t]
            seen_q[r] = seen_q[r] * decay[t]
        fix = beta[t] * (value[t] - seen_k[t])
        corrections.append(fix)
        for r in range(t, NEW):
            if r > t:
                seen_k[r] = seen_k[r] + inner(key_rows[t], key_rows[r]) * fix
            seen_q[r] = seen_q[r] + inner(key_rows[t], query[r]) * fix
    for t in range(NEW):
        o = seen_q[t]
        o = o * lax.rsqrt(jnp.mean(o * o, axis=1, keepdims=True) + epsilon)
        o = o * head_gain[...] * (gate[t] * jax.nn.sigmoid(gate[t]))
        mix_buf[pl.ds(t, heads, stride=NEW), :] = o
    mix_all[me] = mix_buf[...].astype(BF16)

    @pl.loop(1, kv_count)
    def _(off):
        to = lax.rem(me + off, kv_count)
        remote(mix_all.at[me], mix_all.at[me], 1, to, to, me).start()

    u_buf[...] = jnp.zeros_like(u_buf)
    after = jnp.ones((heads, 1), F32)
    for t in range(NEW - 1, -1, -1):
        u_buf[pl.ds(t, heads, stride=8), :] = corrections[t] * after
        after = after * decay[t]
    a_buf[...] = jnp.broadcast_to(after, (heads, TILE))
    for h in range(heads):
        outer = lax.dot_general(
            kq_buf[h * 8 : (h + 1) * 8, :],
            u_buf[h * 8 : (h + 1) * 8, :],
            (((0,), (0,)), ((), ())),
            precision=HIGH,
            preferred_element_type=F32,
        )
        v_mem[h] = v_mem[h] * a_buf[h : h + 1, :] + outer
    store = pltpu.make_async_copy(v_mem, new_memory, load_sem.at[len(pairs)])
    store.start()

    for off in range(1, kv_count):
        src = lax.rem(me + off, kv_count)
        remote(mix_all.at[src], mix_all.at[src], 1, src, src, src).wait_recv()
    gathered = mix_all[...].reshape(slots_wide, DV)
    packed = dot(collect, gathered).astype(BF16)
    loads[5].wait()
    packed = jnp.concatenate(
        [packed[h * compact : (h + 1) * compact, :] for h in range(heads)], axis=1
    )
    attended = tp_swap(0, dot(packed, v_output[...]))
    hidden = (tok_packed + attended).astype(BF16).astype(F32)
    squares = jnp.broadcast_to(
        jnp.sum(hidden * hidden, axis=1, keepdims=True), (compact, TILE)
    )
    sq_send[...] = squares.reshape(groups, GROUP, TILE)

    @pl.loop(1, kv_count)
    def _(off):
        to = lax.rem(me + off, kv_count)
        remote(sq_send.at[lax.rem(to, groups)], sq_recv.at[me], 2, to, to, me).start()

    hscaled = hidden * mlp_gain[...]
    blank = jnp.zeros((GROUP, width), F32)
    gate_rows, up_rows = [], []
    for g in range(groups):
        own = hscaled[g * GROUP : (g + 1) * GROUP, :]
        gate_rows += [own, blank]
        up_rows += [blank, own]
    gate_rows = jnp.concatenate(gate_rows, axis=0).astype(BF16)
    up_rows = jnp.concatenate(up_rows, axis=0).astype(BF16)
    loads[6].wait()
    loads[7].wait()
    zone_me = me // groups
    zone_order = [2, 1, 3, 0] if zones == 4 else list(range(zones))
    for step in zone_order:
        zone = lax.rem(zone_me + step, zones)
        cols = pl.ds(pl.multiple_of(zone * chunk, TILE), chunk)
        term = dot(gate_rows, v_gate[:, cols]) + dot(up_rows, v_up[:, cols])
        gu_send[pl.ds(zone * groups, groups)] = term.astype(BF16).reshape(
            groups, 2 * GROUP, chunk
        )

        for g in range(groups):
            if step == 0:
                if g == 0:
                    continue
                to = zone * groups + lax.rem(me + g, groups)
            else:
                to = zone * groups + lax.rem(me + g, groups)
            remote(gu_send.at[to], gu_recv.at[me], 3, to, to, me).start()

    def sources():
        for step in [0, 1, 3, 2] if zones == 4 else range(zones):
            for g in range(groups):
                if step or g:
                    yield lax.rem(zone_me + step, zones) * groups + lax.rem(me + g, groups)

    mean_sq = sq_send[lax.rem(me, groups)]
    for src in sources():
        remote(sq_send.at[0], sq_recv.at[src], 2, src, src, src).wait_recv()
        mean_sq = mean_sq + sq_recv[src]
    rstd2 = lax.rsqrt(mean_sq / total_width + epsilon)[:, :1]
    both = gu_send[me].astype(F32)
    for src in sources():
        remote(gu_send.at[src], gu_recv.at[src], 3, src, src, src).wait_recv()
        both = both + gu_recv[src].astype(F32)
    gated = both[:GROUP] * rstd2
    active = gated * jax.nn.sigmoid(gated) * (both[GROUP:] * rstd2)
    act_all[me] = active.astype(BF16)
    for step in zone_order:
        for g in range(groups):
            if step or g:
                to = lax.rem(zone_me + step, zones) * groups + lax.rem(me + g, groups)
                remote(act_all.at[me], act_all.at[me], 4, to, to, me).start()
    loads[8].wait()
    feed = jnp.zeros((compact, width), F32)
    for step in [0, 1, 3, 2] if zones == 4 else range(zones):
        zone = lax.rem(zone_me + step, zones)
        for g in range(groups):
            if step or g:
                src = zone * groups + lax.rem(me + g, groups)
                remote(act_all.at[src], act_all.at[src], 4, src, src, src).wait_recv()
        part = act_all[pl.ds(zone * groups, groups)].astype(F32).reshape(compact, chunk)
        cols = pl.ds(pl.multiple_of(zone * chunk, TILE), chunk)
        feed = feed + dot(part.astype(BF16), v_down[cols, :])
    result = (hidden + tp_swap(1, feed)).astype(BF16)
    out[...] = dot(unpack, result).astype(BF16)

    store.wait()

    @pl.loop(1, kv_count)
    def _(off):
        to = lax.rem(me + off, kv_count)
        remote(proj_send.at[to], proj_recv.at[me], 0, to, to, me).wait_send()
        remote(mix_all.at[me], mix_all.at[me], 1, to, to, me).wait_send()
        remote(sq_send.at[0], sq_recv.at[me], 2, to, to, me).wait_send()
        remote(gu_send.at[to], gu_recv.at[me], 3, to, to, me).wait_send()
        remote(act_all.at[me], act_all.at[me], 4, to, to, me).wait_send()


def fused_device(
    tokens,
    lengths,
    memory,
    norm_gain,
    w_query,
    w_key,
    w_value,
    w_outgate,
    w_alpha,
    w_beta,
    decay_log,
    decay_bias,
    head_gain,
    w_output,
    mlp_gain,
    w_gate,
    w_up,
    w_down,
):
    kv_count = lax.axis_size("kv")
    rows, width = tokens.shape
    heads = memory.shape[1]
    live_rows = (rows // NEW) * 7 // 4
    compact = -(-live_rows // 16) * 16
    groups = compact // GROUP
    zones = kv_count // groups
    chunk = w_gate.shape[1] // zones
    wide = heads * DV
    vmem = pl.BlockSpec(memory_space=pltpu.VMEM)
    far = pl.BlockSpec(memory_space=pl.ANY)
    out, state = pl.pallas_call(
        fused,
        out_shape=(
            jax.ShapeDtypeStruct((rows, width), BF16),
            jax.ShapeDtypeStruct(memory.shape[1:], F32),
        ),
        in_specs=[pl.BlockSpec(memory_space=pltpu.SMEM)] + [vmem] * 8 + [far] * 9,
        out_specs=(vmem, far),
        scratch_shapes=[
            pltpu.VMEM(memory.shape[1:], F32),
            pltpu.VMEM(w_query.shape, BF16),
            pltpu.VMEM(w_key.shape, BF16),
            pltpu.VMEM(w_value.shape, BF16),
            pltpu.VMEM(w_outgate.shape, BF16),
            pltpu.VMEM(w_output.shape, BF16),
            pltpu.VMEM(w_gate.shape, BF16),
            pltpu.VMEM(w_up.shape, BF16),
            pltpu.VMEM(w_down.shape, BF16),
            pltpu.VMEM((kv_count, 16, wide + TILE), BF16),
            pltpu.VMEM((kv_count, 16, wide + TILE), BF16),
            pltpu.VMEM((16, TILE), F32),
            pltpu.VMEM((heads * 16, TILE), F32),
            pltpu.VMEM((heads * 8, TILE), F32),
            pltpu.VMEM((heads * 8, TILE), F32),
            pltpu.VMEM((heads * 8, TILE), F32),
            pltpu.VMEM((heads, TILE), F32),
            pltpu.VMEM((16, TILE), F32),
            pltpu.VMEM((heads * NEW, TILE), F32),
            pltpu.VMEM((kv_count, heads * NEW, TILE), BF16),
            pltpu.VMEM((2, compact, width), F32),
            pltpu.VMEM((2, compact, width), F32),
            pltpu.VMEM((groups, GROUP, TILE), F32),
            pltpu.VMEM((kv_count, GROUP, TILE), F32),
            pltpu.VMEM((kv_count, 2 * GROUP, chunk), BF16),
            pltpu.VMEM((kv_count, 2 * GROUP, chunk), BF16),
            pltpu.VMEM((kv_count, GROUP, chunk), BF16),
            pltpu.SemaphoreType.DMA((10,)),
            pltpu.SemaphoreType.DMA((5, kv_count)),
            pltpu.SemaphoreType.DMA((5, kv_count)),
            pltpu.SemaphoreType.DMA((2, 2)),
        ],
        compiler_params=pltpu.CompilerParams(
            collective_id=0, has_side_effects=True, vmem_limit_bytes=48 * 1024 * 1024
        ),
    )(
        lengths,
        tokens,
        norm_gain.reshape(1, -1),
        decay_log.reshape(1, -1),
        decay_bias.reshape(1, -1),
        head_gain.reshape(1, -1),
        mlp_gain.reshape(1, -1),
        w_alpha,
        w_beta,
        memory.reshape(memory.shape[1:]),
        w_query,
        w_key,
        w_value,
        w_outgate,
        w_output,
        w_gate,
        w_up,
        w_down,
    )
    return out, state.reshape(memory.shape)


def fits(tokens, memory, w_gate):
    kv_count = lax.axis_size("kv")
    rows, width = tokens.shape
    live_rows = (rows // NEW) * 7 // 4
    groups = -(-live_rows // 16) * 16 // GROUP
    return (
        lax.axis_size("tp") == 2
        and memory.shape[0] == 1
        and memory.shape[1] == 8
        and rows == kv_count * NEW
        and rows % 16 == 0
        and width % TILE == 0
        and kv_count % groups == 0
        and w_gate.shape[1] % (kv_count // groups * TILE) == 0
    )


def layer(*arrays):
    if fits(arrays[0], arrays[2], arrays[15]):
        return fused_device(*arrays)
    return per_device(*arrays)


def solution(mesh):
    placed = (
        P(None, "kv"),
        P(),
        P("kv", "tp", None, None),
        P("kv"),
        P("kv", "tp"),
        P("kv", "tp"),
        P("kv", "tp"),
        P("kv", "tp"),
        P("kv", None),
        P("kv", None),
        P("tp"),
        P("tp"),
        P(),
        P("tp", "kv"),
        P("kv"),
        P("kv", "tp"),
        P("kv", "tp"),
        P("tp", "kv"),
    )
    return jax.shard_map(
        layer,
        mesh=mesh,
        in_specs=placed,
        out_specs=(P(None, "kv"), P("kv", "tp", None, None)),
        check_vma=False,
    )
```

```python
import jax
import jax.numpy as jnp
from jax import lax
from jax.experimental import pallas as pl
from jax.experimental.pallas import tpu as pltpu
from jax.sharding import PartitionSpec as P

D = 4096
DK = 128
DV = 128
NEW = 4


epsilon = 1e-06


def unit_rows(values):
    return values * lax.rsqrt(jnp.sum(values * values, axis=-1, keepdims=True) + epsilon)


def advance(memory, queries, key_rows, value_rows, decays, betas):
    outputs = []
    for step in range(queries.shape[1]):
        memory = jnp.exp(decays[:, step])[:, :, None, None] * memory
        predicted = jnp.einsum(
            "shde,shd->she", memory, key_rows[:, step], precision=lax.Precision.HIGHEST
        )
        correction = betas[:, step][:, :, None] * (value_rows[:, step] - predicted)
        memory = memory + key_rows[:, step][:, :, :, None] * correction[:, :, None, :]
        outputs.append(
            jnp.einsum("shde,shd->she", memory, queries[:, step], precision=lax.Precision.HIGHEST)
        )
    return (memory, jnp.stack(outputs, axis=1))


def per_device(
    tokens,
    lengths,
    memory,
    norm_gain,
    w_query,
    w_key,
    w_value,
    w_outgate,
    w_alpha,
    w_beta,
    decay_log,
    decay_bias,
    head_gain,
    w_output,
    mlp_gain,
    w_gate,
    w_up,
    w_down,
):
    total_rows = tokens.shape[0]
    kv_count = lax.axis_size("kv")
    kv_place = lax.axis_index("kv")
    tp_place = lax.axis_index("tp")
    own_rows = total_rows // kv_count
    seq_dev = memory.shape[0]
    heads_dev = memory.shape[1]
    token_f = tokens.astype(jnp.float32)
    squares = jnp.sum(token_f * token_f, axis=1)
    scaled = (token_f * norm_gain).astype(jnp.bfloat16)
    part_query = jnp.dot(scaled, w_query, preferred_element_type=jnp.float32)
    part_key = jnp.dot(scaled, w_key, preferred_element_type=jnp.float32)
    part_value = jnp.dot(scaled, w_value, preferred_element_type=jnp.float32)
    part_gate = jnp.dot(scaled, w_outgate, preferred_element_type=jnp.float32)
    part_alpha = jnp.dot(scaled, w_alpha, preferred_element_type=jnp.float32)
    part_beta = jnp.dot(scaled, w_beta, preferred_element_type=jnp.float32)
    all_squares = lax.psum(squares, "kv")
    sum_query, sum_key, sum_value, sum_gate, sum_alpha, sum_beta = (
        lax.psum_scatter(part_query, "kv", scatter_dimension=0, tiled=True),
        lax.psum_scatter(part_key, "kv", scatter_dimension=0, tiled=True),
        lax.psum_scatter(part_value, "kv", scatter_dimension=0, tiled=True),
        lax.psum_scatter(part_gate, "kv", scatter_dimension=0, tiled=True),
        lax.psum_scatter(part_alpha, "kv", scatter_dimension=0, tiled=True),
        lax.psum_scatter(part_beta, "kv", scatter_dimension=0, tiled=True),
    )
    own_squares = lax.dynamic_slice_in_dim(all_squares, kv_place * own_rows, own_rows)
    rstd = lax.rsqrt(own_squares / D + epsilon)[:, None]
    queries = (sum_query * rstd).astype(jnp.bfloat16)
    key_rows = (sum_key * rstd).astype(jnp.bfloat16)
    value_rows = (sum_value * rstd).astype(jnp.bfloat16)
    outgate = (sum_gate * rstd).astype(jnp.bfloat16)
    alphas = lax.dynamic_slice_in_dim(sum_alpha * rstd, tp_place * heads_dev, heads_dev, 1)
    beta_pre = lax.dynamic_slice_in_dim(sum_beta * rstd, tp_place * heads_dev, heads_dev, 1)
    own_lengths = lax.dynamic_slice_in_dim(lengths, kv_place * seq_dev, seq_dev)
    live = jnp.arange(NEW, dtype=jnp.int32)[None, :] < own_lengths[:, None]
    query_h = unit_rows(queries.astype(jnp.float32).reshape(seq_dev, NEW, heads_dev, DK)) * DK ** (
        -0.5
    )
    key_h = unit_rows(key_rows.astype(jnp.float32).reshape(seq_dev, NEW, heads_dev, DK))
    value_h = value_rows.astype(jnp.float32).reshape(seq_dev, NEW, heads_dev, DV)
    decays = -jnp.exp(decay_log) * jax.nn.softplus(alphas + decay_bias)
    decays = jnp.where(live[:, :, None], decays.reshape(seq_dev, NEW, heads_dev), 0.0)
    betas = jnp.where(
        live[:, :, None], jax.nn.sigmoid(beta_pre).reshape(seq_dev, NEW, heads_dev), 0.0
    )
    new_memory, attended = advance(memory, query_h, key_h, value_h, decays, betas)
    attended = attended * lax.rsqrt(jnp.mean(attended * attended, axis=-1, keepdims=True) + epsilon)
    gate_h = outgate.astype(jnp.float32).reshape(seq_dev, NEW, heads_dev, DV)
    mixed = (
        (attended * head_gain * jax.nn.silu(gate_h))
        .astype(jnp.bfloat16)
        .reshape(own_rows, heads_dev * DV)
    )
    attn_terms = jnp.dot(
        lax.all_gather(mixed, "kv", axis=0, tiled=True),
        w_output,
        preferred_element_type=jnp.float32,
    )
    attn_total = lax.psum(attn_terms, "tp")
    hidden = (token_f + attn_total).astype(jnp.bfloat16)
    hidden_f = hidden.astype(jnp.float32)
    hidden_squares = jnp.sum(hidden_f * hidden_f, axis=1)
    hscaled = (hidden_f * mlp_gain).astype(jnp.bfloat16)
    all_live = (jnp.arange(NEW, dtype=jnp.int32)[None, :] < lengths[:, None]).reshape(total_rows)
    part_gate_rows = jnp.dot(hscaled, w_gate, preferred_element_type=jnp.float32)
    part_up_rows = jnp.dot(hscaled, w_up, preferred_element_type=jnp.float32)
    gate_rows, up_rows, mlp_squares = lax.psum((part_gate_rows, part_up_rows, hidden_squares), "kv")
    rstd2 = lax.rsqrt(mlp_squares / D + epsilon)[:, None]
    active = (jax.nn.silu(gate_rows * rstd2) * (up_rows * rstd2)).astype(jnp.bfloat16)
    feed_terms = jnp.dot(active, w_down, preferred_element_type=jnp.float32)
    feed_total = lax.psum(feed_terms.astype(jnp.bfloat16), "tp").astype(jnp.float32)
    layer_out = jnp.where(all_live[:, None], hidden_f + feed_total, 0.0).astype(jnp.bfloat16)
    return (layer_out, new_memory)


F32 = jnp.float32
BF16 = jnp.bfloat16
HIGH = lax.Precision.HIGHEST
TILE = 128
GROUP = 8


def iota(shape, axis):
    return lax.broadcasted_iota(jnp.int32, shape, axis)


def dot(a, b, precision=None):
    return jnp.dot(a, b, preferred_element_type=F32, precision=precision)


def fused(
    lens,
    tokens,
    norm_gain,
    decay_log,
    decay_bias,
    head_gain,
    mlp_gain,
    w_alpha,
    w_beta,
    memory,
    w_query,
    w_key,
    w_value,
    w_outgate,
    w_output,
    w_gate,
    w_up,
    w_down,
    out,
    new_memory,
    v_mem,
    v_query,
    v_key,
    v_value,
    v_outgate,
    v_output,
    v_gate,
    v_up,
    v_down,
    proj_send,
    proj_recv,
    proj_part,
    proj_last,
    small_send,
    small_recv,
    rs_buf,
    xs_buf,
    kq_buf,
    r_buf,
    u_buf,
    a_buf,
    ab_buf,
    mix_buf,
    mix_all,
    tp_send,
    tp_recv,
    sq_send,
    sq_recv,
    gu_send,
    gu_recv,
    gu_part,
    gu_last,
    act_all,
    load_sem,
    send_sem,
    recv_sem,
    tp_sem,
):
    kv_count = mix_all.shape[0]
    me = lax.axis_index("kv")
    tp = lax.axis_index("tp")
    rows, width = tokens.shape
    heads = v_mem.shape[0]
    wide = heads * DV
    compact = tp_send.shape[1]
    groups = compact // GROUP
    zones = kv_count // groups
    chunk = gu_send.shape[2]
    total_width = width * kv_count

    barrier = pltpu.get_barrier_semaphore()

    @pl.loop(1, kv_count)
    def _(off):
        pl.semaphore_signal(
            barrier,
            inc=1,
            device_id={"kv": lax.rem(me + off, kv_count)},
            device_id_type=pl.DeviceIdType.MESH,
        )

    pl.semaphore_signal(
        barrier, inc=1, device_id={"tp": 1 - tp}, device_id_type=pl.DeviceIdType.MESH
    )
    pairs = [
        (w_query, v_query),
        (w_key, v_key),
        (w_value, v_value),
        (w_outgate, v_outgate),
        (memory, v_mem),
        (w_output, v_output),
        (w_gate, v_gate),
        (w_up, v_up),
        (w_down, v_down),
    ]
    loads = [pltpu.make_async_copy(a, b, load_sem.at[n]) for n, (a, b) in enumerate(pairs)]
    for load in loads:
        load.start()

    def remote(src, dst, phase, slot, partner, arrival):
        return pltpu.make_async_remote_copy(
            src_ref=src,
            dst_ref=dst,
            send_sem=send_sem.at[phase, slot],
            recv_sem=recv_sem.at[phase, arrival],
            device_id={"kv": partner},
            device_id_type=pl.DeviceIdType.MESH,
        )

    def tp_swap(phase, value):
        tp_send[phase] = value
        swap = pltpu.make_async_remote_copy(
            src_ref=tp_send.at[phase],
            dst_ref=tp_recv.at[phase],
            send_sem=tp_sem.at[phase, 0],
            recv_sem=tp_sem.at[phase, 1],
            device_id={"tp": 1 - tp},
            device_id_type=pl.DeviceIdType.MESH,
        )
        swap.start()
        swap.wait()
        return value + tp_recv[phase]

    all_rows = kv_count * 4 * NEW
    row = iota((all_rows, rows), 0)
    spread = jnp.where(
        iota((all_rows, rows), 1) == (row >> 4) * NEW + (row & 3), 1.0, 0.0
    ).astype(BF16)
    tok = tokens[...]
    scaled = (tok.astype(F32) * norm_gain[...]).astype(BF16)
    wide_tok = dot(spread, tok)
    wide_scaled = dot(spread, scaled)
    squares = jnp.sum(wide_tok * wide_tok, axis=1, keepdims=True)
    part_of = (iota((all_rows, width), 0) >> 2) & 3
    all_heads = w_alpha.shape[0]
    place = iota((TILE, all_heads), 0)
    head_of = iota((TILE, all_heads), 1)
    w_small = dot(jnp.where(place == head_of, 1.0, 0.0).astype(BF16), w_alpha[...]) + dot(
        jnp.where(place == head_of + all_heads, 1.0, 0.0).astype(BF16), w_beta[...]
    )
    small = lax.dot_general(
        wide_scaled.astype(BF16),
        w_small.astype(BF16),
        (((1,), (1,)), ((), ())),
        preferred_element_type=F32,
    )
    lane = iota((all_rows, TILE), 1)
    small = jnp.where(lane == 2 * all_heads, squares, small)
    small_send[...] = small.reshape(kv_count, 16, TILE)[:, :GROUP, :]
    masked = [jnp.where(part_of == p, wide_scaled, 0.0).astype(BF16) for p in range(4)]
    for load in loads[:4]:
        load.wait()
    half = wide // 2
    for c in range(2):
        cols = slice(c * half, (c + 1) * half)
        acc = dot(masked[0], v_query[:, cols])
        acc = acc + dot(masked[1], v_key[:, cols])
        acc = acc + dot(masked[2], v_value[:, cols])
        acc = acc + dot(masked[3], v_outgate[:, cols])
        proj_send[:, :, cols] = acc.astype(BF16).reshape(kv_count, 16, half)

    pl.semaphore_wait(barrier, kv_count)

    zone_me = me // groups
    group_me = lax.rem(me, groups)
    steps = [2, 1, 3, 0] if zones == 4 else [*range(1, zones), 0]

    def zone_of(step):
        return lax.rem(zone_me + step, zones)

    def peer(g):
        return lax.rem(group_me + g, groups)

    def send_plane(send, recv, phase, zone):
        for g in range(1, groups):
            slab = zone * groups + peer(g)
            remote(
                send.at[slab],
                recv.at[zone * groups + group_me],
                phase,
                slab,
                zone_me * groups + peer(g),
                zone * groups + group_me,
            ).start()

    def sum_plane(send, recv, phase, zone):
        added = send[zone * groups + group_me].astype(F32)
        for g in range(1, groups):
            slab = zone * groups + peer(g)
            remote(send.at[slab], recv.at[slab], phase, slab, me, slab).wait_recv()
            added = added + recv[slab].astype(F32)
        return added

    def reduce_kv(send, recv, part, last, phase):
        for step in steps[:-1]:
            zone = zone_of(step)
            part[zone] = sum_plane(send, recv, phase, zone).astype(BF16)
            remote(
                part.at[zone],
                last.at[zone_me],
                phase + 1,
                zone,
                zone * groups + group_me,
                zone_me,
            ).start()
        added = sum_plane(send, recv, phase, zone_me)
        for step in steps[:-1][::-1]:
            zone = zone_of(step)
            remote(part.at[zone], last.at[zone], phase + 1, zone, me, zone).wait_recv()
            added = added + last[zone].astype(F32)
        return added

    @pl.loop(1, kv_count)
    def _(off):
        to = lax.rem(me + off, kv_count)
        remote(small_send.at[to], small_recv.at[me], 5, to, to, me).start()

    for step in steps:
        send_plane(proj_send, proj_recv, 0, zone_of(step))

    slots_wide = kv_count * heads * NEW
    shape_a = (1, rows)
    shape_b = (1, slots_wide)
    shape_c = (rows, compact)
    length_a = jnp.zeros(shape_a, jnp.int32)
    start_a = jnp.zeros(shape_a, jnp.int32)
    length_b = jnp.zeros(shape_b, jnp.int32)
    start_b = jnp.zeros(shape_b, jnp.int32)
    length_c = jnp.zeros(shape_c, jnp.int32)
    start_c = jnp.zeros(shape_c, jnp.int32)
    seq_a = iota(shape_a, 1) >> 2
    seq_b = iota(shape_b, 1) >> 5
    seq_c = iota(shape_c, 0) >> 2
    begin = jnp.int32(0)
    for s in range(kv_count):
        length_a = jnp.where(seq_a == s, lens[s], length_a)
        start_a = jnp.where(seq_a == s, begin, start_a)
        length_b = jnp.where(seq_b == s, lens[s], length_b)
        start_b = jnp.where(seq_b == s, begin, start_b)
        length_c = jnp.where(seq_c == s, lens[s], length_c)
        start_c = jnp.where(seq_c == s, begin, start_c)
        begin = begin + lens[s]
    slot_a = iota(shape_a, 1) & 3
    rank_a = jnp.where(slot_a < length_a, start_a + slot_a, -1)
    pack = jnp.where(rank_a == iota((compact, rows), 0), 1.0, 0.0).astype(BF16)
    slot_c = iota(shape_c, 0) & 3
    rank_c = jnp.where(slot_c < length_c, start_c + slot_c, -1)
    unpack = jnp.where(rank_c == iota(shape_c, 1), 1.0, 0.0).astype(BF16)
    slot_b = iota(shape_b, 1) & 3
    head_b = (iota(shape_b, 1) >> 2) & (heads - 1)
    rank_b = jnp.where(slot_b < length_b, head_b * compact + start_b + slot_b, -1)
    collect = jnp.where(rank_b == iota((heads * compact, slots_wide), 0), 1.0, 0.0).astype(BF16)
    tok_packed = dot(pack, tok)

    small = small_send[me]
    for off in range(1, kv_count):
        src = lax.rem(me + off, kv_count)
        remote(small_send.at[src], small_recv.at[src], 5, src, src, src).wait_recv()
        small = small + small_recv[src]
    small = small[:NEW]
    total = reduce_kv(proj_send, proj_recv, proj_part, proj_last, 0)
    lane = iota((NEW, TILE), 1)
    mean_sq = jnp.sum(jnp.where(lane == 2 * all_heads, small, 0.0), axis=1, keepdims=True)
    rstd = lax.rsqrt(mean_sq / total_width + epsilon)
    rstd_wide = jnp.broadcast_to(rstd, (NEW, TILE))
    small = small * rstd
    ab_buf[0:4, :] = small
    for p in range(4):
        rs_buf[p * NEW : (p + 1) * NEW, :] = rstd_wide
    scale = rs_buf[...]
    for h in range(heads):
        piece = total[:, h * DV : (h + 1) * DV] * scale
        xs_buf[h * 16 : (h + 1) * 16, :] = piece.astype(BF16).astype(F32)

    def slot_rows(ref, index, stride):
        return ref[pl.ds(index, heads, stride=stride), :]

    query, key_rows, value, gate = (
        [slot_rows(xs_buf, p * NEW + t, 16) for t in range(NEW)] for p in range(4)
    )
    query = [unit_rows(x) * DK ** (-0.5) for x in query]
    key_rows = [unit_rows(x) for x in key_rows]
    eye = iota((heads, heads), 0) == iota((heads, heads), 1)
    rate = jnp.sum(jnp.where(eye, jnp.exp(decay_log[...]), 0.0), axis=1, keepdims=True)
    bias = jnp.sum(jnp.where(eye, decay_bias[...], 0.0), axis=1, keepdims=True)
    pick = iota((heads, TILE), 1) - iota((heads, TILE), 0)
    own_length = jnp.full((heads, 1), lens[me], jnp.int32)
    decay, beta = [], []
    for t in range(NEW):
        line = ab_buf[t : t + 1, :]
        alpha = jnp.sum(jnp.where(pick == tp * heads, line, 0.0), axis=1, keepdims=True)
        write = jnp.sum(
            jnp.where(pick == tp * heads + all_heads, line, 0.0), axis=1, keepdims=True
        )
        x = alpha + bias
        soft = jnp.maximum(x, 0.0) + jnp.log1p(jnp.exp(-jnp.abs(x)))
        live = own_length > t
        decay.append(jnp.exp(jnp.where(live, -rate * soft, 0.0)))
        beta.append(jnp.where(live, jax.nn.sigmoid(write), 0.0))
    for t in range(NEW):
        kq_buf[pl.ds(t, heads, stride=8), :] = key_rows[t]
        kq_buf[pl.ds(NEW + t, heads, stride=8), :] = query[t]
    loads[4].wait()
    for h in range(heads):
        r_buf[h * 8 : (h + 1) * 8, :] = dot(kq_buf[h * 8 : (h + 1) * 8, :], v_mem[h], HIGH)
    seen_k = [slot_rows(r_buf, t, 8) for t in range(NEW)]
    seen_q = [slot_rows(r_buf, NEW + t, 8) for t in range(NEW)]

    def inner(a, b):
        return jnp.sum(a * b, axis=1, keepdims=True)

    corrections = []
    for t in range(NEW):
        for r in range(t, NEW):
            seen_k[r] = seen_k[r] * decay[t]
            seen_q[r] = seen_q[r] * decay[t]
        fix = beta[t] * (value[t] - seen_k[t])
        corrections.append(fix)
        for r in range(t, NEW):
            if r > t:
                seen_k[r] = seen_k[r] + inner(key_rows[t], key_rows[r]) * fix
            seen_q[r] = seen_q[r] + inner(key_rows[t], query[r]) * fix
    for t in range(NEW):
        o = seen_q[t]
        o = o * lax.rsqrt(jnp.mean(o * o, axis=1, keepdims=True) + epsilon)
        o = o * head_gain[...] * (gate[t] * jax.nn.sigmoid(gate[t]))
        mix_buf[pl.ds(t, heads, stride=NEW), :] = o
    mix_all[me] = mix_buf[...].astype(BF16)

    @pl.loop(1, kv_count)
    def _(off):
        to = lax.rem(me + off, kv_count)
        remote(mix_all.at[me], mix_all.at[me], 2, to, to, me).start()

    u_buf[...] = jnp.zeros_like(u_buf)
    after = jnp.ones((heads, 1), F32)
    for t in range(NEW - 1, -1, -1):
        u_buf[pl.ds(t, heads, stride=8), :] = corrections[t] * after
        after = after * decay[t]
    a_buf[...] = jnp.broadcast_to(after, (heads, TILE))
    for h in range(heads):
        outer = lax.dot_general(
            kq_buf[h * 8 : (h + 1) * 8, :],
            u_buf[h * 8 : (h + 1) * 8, :],
            (((0,), (0,)), ((), ())),
            precision=HIGH,
            preferred_element_type=F32,
        )
        v_mem[h] = v_mem[h] * a_buf[h : h + 1, :] + outer
    store = pltpu.make_async_copy(v_mem, new_memory, load_sem.at[len(pairs)])
    store.start()

    for off in range(1, kv_count):
        src = lax.rem(me + off, kv_count)
        remote(mix_all.at[src], mix_all.at[src], 2, src, src, src).wait_recv()
    gathered = mix_all[...].reshape(slots_wide, DV)
    packed = dot(collect, gathered).astype(BF16)
    loads[5].wait()
    packed = jnp.concatenate(
        [packed[h * compact : (h + 1) * compact, :] for h in range(heads)], axis=1
    )
    attended = tp_swap(0, dot(packed, v_output[...]))
    hidden = (tok_packed + attended).astype(BF16).astype(F32)
    squares = jnp.broadcast_to(
        jnp.sum(hidden * hidden, axis=1, keepdims=True), (compact, TILE)
    )
    sq_send[...] = squares.reshape(groups, GROUP, TILE)

    @pl.loop(1, kv_count)
    def _(off):
        to = lax.rem(me + off, kv_count)
        remote(sq_send.at[lax.rem(to, groups)], sq_recv.at[me], 6, to, to, me).start()

    hscaled = hidden * mlp_gain[...]
    blank = jnp.zeros((GROUP, width), F32)
    gate_rows, up_rows = [], []
    for g in range(groups):
        own = hscaled[g * GROUP : (g + 1) * GROUP, :]
        gate_rows += [own, blank]
        up_rows += [blank, own]
    gate_rows = jnp.concatenate(gate_rows, axis=0).astype(BF16)
    up_rows = jnp.concatenate(up_rows, axis=0).astype(BF16)
    loads[6].wait()
    loads[7].wait()
    for step in steps:
        zone = zone_of(step)
        cols = pl.ds(pl.multiple_of(zone * chunk, TILE), chunk)
        term = dot(gate_rows, v_gate[:, cols]) + dot(up_rows, v_up[:, cols])
        gu_send[pl.ds(zone * groups, groups)] = term.astype(BF16).reshape(
            groups, 2 * GROUP, chunk
        )
        send_plane(gu_send, gu_recv, 3, zone)
    mean_sq = sq_send[group_me]
    for off in range(1, kv_count):
        src = lax.rem(me + off, kv_count)
        remote(sq_send.at[0], sq_recv.at[src], 6, src, src, src).wait_recv()
        mean_sq = mean_sq + sq_recv[src]
    rstd2 = lax.rsqrt(mean_sq / total_width + epsilon)[:, :1]
    both = reduce_kv(gu_send, gu_recv, gu_part, gu_last, 3)
    gated = both[:GROUP] * rstd2
    active = gated * jax.nn.sigmoid(gated) * (both[GROUP:] * rstd2)
    act_all[me] = active.astype(BF16)

    def pass_on(zone, slot, partner):
        block = zone * groups + group_me
        remote(act_all.at[block], act_all.at[block], 7, slot, partner, block).start()

    def arrive(block):
        remote(act_all.at[block], act_all.at[block], 7, block, me, block).wait_recv()

    def forward(zone):
        for g in range(1, groups):
            pass_on(zone, zone * groups + peer(g), zone_me * groups + peer(g))

    for step in steps[:-1]:
        there = zone_of(step) * groups + group_me
        pass_on(zone_me, there, there)
    forward(zone_me)
    near_first = [0, 1, 3, 2] if zones == 4 else list(range(zones))
    for step in near_first[1:]:
        zone = zone_of(step)
        arrive(zone * groups + group_me)
        forward(zone)
    loads[8].wait()
    feed = jnp.zeros((compact, width), F32)
    for step in near_first:
        zone = zone_of(step)
        for g in range(1, groups):
            arrive(zone * groups + peer(g))
        part = act_all[pl.ds(zone * groups, groups)].astype(F32).reshape(compact, chunk)
        cols = pl.ds(pl.multiple_of(zone * chunk, TILE), chunk)
        feed = feed + dot(part.astype(BF16), v_down[cols, :])
    result = (hidden + tp_swap(1, feed)).astype(BF16)
    out[...] = dot(unpack, result).astype(BF16)

    store.wait()

    @pl.loop(1, kv_count)
    def _(off):
        to = lax.rem(me + off, kv_count)
        remote(mix_all.at[me], mix_all.at[me], 2, to, to, me).wait_send()
        remote(small_send.at[to], small_recv.at[me], 5, to, to, me).wait_send()
        remote(sq_send.at[0], sq_recv.at[me], 6, to, to, me).wait_send()
        remote(act_all.at[me], act_all.at[me], 7, to, to, me).wait_send()

    for step in steps:
        zone = zone_of(step)
        for g in range(1, groups):
            slab = zone * groups + peer(g)
            remote(proj_send.at[slab], proj_recv.at[slab], 0, slab, me, slab).wait_send()
            remote(gu_send.at[slab], gu_recv.at[slab], 3, slab, me, slab).wait_send()
        if step:
            remote(proj_part.at[zone], proj_last.at[zone], 1, zone, me, zone).wait_send()
            remote(gu_part.at[zone], gu_last.at[zone], 4, zone, me, zone).wait_send()


def fused_device(
    tokens,
    lengths,
    memory,
    norm_gain,
    w_query,
    w_key,
    w_value,
    w_outgate,
    w_alpha,
    w_beta,
    decay_log,
    decay_bias,
    head_gain,
    w_output,
    mlp_gain,
    w_gate,
    w_up,
    w_down,
):
    kv_count = lax.axis_size("kv")
    rows, width = tokens.shape
    heads = memory.shape[1]
    live_rows = (rows // NEW) * 7 // 4
    compact = -(-live_rows // 16) * 16
    groups = compact // GROUP
    zones = kv_count // groups
    chunk = w_gate.shape[1] // zones
    wide = heads * DV
    vmem = pl.BlockSpec(memory_space=pltpu.VMEM)
    far = pl.BlockSpec(memory_space=pl.ANY)
    out, state = pl.pallas_call(
        fused,
        out_shape=(
            jax.ShapeDtypeStruct((rows, width), BF16),
            jax.ShapeDtypeStruct(memory.shape[1:], F32),
        ),
        in_specs=[pl.BlockSpec(memory_space=pltpu.SMEM)] + [vmem] * 8 + [far] * 9,
        out_specs=(vmem, far),
        scratch_shapes=[
            pltpu.VMEM(memory.shape[1:], F32),
            pltpu.VMEM(w_query.shape, BF16),
            pltpu.VMEM(w_key.shape, BF16),
            pltpu.VMEM(w_value.shape, BF16),
            pltpu.VMEM(w_outgate.shape, BF16),
            pltpu.VMEM(w_output.shape, BF16),
            pltpu.VMEM(w_gate.shape, BF16),
            pltpu.VMEM(w_up.shape, BF16),
            pltpu.VMEM(w_down.shape, BF16),
            pltpu.VMEM((kv_count, 16, wide), BF16),
            pltpu.VMEM((kv_count, 16, wide), BF16),
            pltpu.VMEM((zones, 16, wide), BF16),
            pltpu.VMEM((zones, 16, wide), BF16),
            pltpu.VMEM((kv_count, GROUP, TILE), F32),
            pltpu.VMEM((kv_count, GROUP, TILE), F32),
            pltpu.VMEM((16, TILE), F32),
            pltpu.VMEM((heads * 16, TILE), F32),
            pltpu.VMEM((heads * 8, TILE), F32),
            pltpu.VMEM((heads * 8, TILE), F32),
            pltpu.VMEM((heads * 8, TILE), F32),
            pltpu.VMEM((heads, TILE), F32),
            pltpu.VMEM((16, TILE), F32),
            pltpu.VMEM((heads * NEW, TILE), F32),
            pltpu.VMEM((kv_count, heads * NEW, TILE), BF16),
            pltpu.VMEM((2, compact, width), F32),
            pltpu.VMEM((2, compact, width), F32),
            pltpu.VMEM((groups, GROUP, TILE), F32),
            pltpu.VMEM((kv_count, GROUP, TILE), F32),
            pltpu.VMEM((kv_count, 2 * GROUP, chunk), BF16),
            pltpu.VMEM((kv_count, 2 * GROUP, chunk), BF16),
            pltpu.VMEM((zones, 2 * GROUP, chunk), BF16),
            pltpu.VMEM((zones, 2 * GROUP, chunk), BF16),
            pltpu.VMEM((kv_count, GROUP, chunk), BF16),
            pltpu.SemaphoreType.DMA((10,)),
            pltpu.SemaphoreType.DMA((8, kv_count)),
            pltpu.SemaphoreType.DMA((8, kv_count)),
            pltpu.SemaphoreType.DMA((2, 2)),
        ],
        compiler_params=pltpu.CompilerParams(
            collective_id=0, has_side_effects=True, vmem_limit_bytes=67043328
        ),
    )(
        lengths,
        tokens,
        norm_gain.reshape(1, -1),
        decay_log.reshape(1, -1),
        decay_bias.reshape(1, -1),
        head_gain.reshape(1, -1),
        mlp_gain.reshape(1, -1),
        w_alpha.T,
        w_beta.T,
        memory.reshape(memory.shape[1:]),
        w_query,
        w_key,
        w_value,
        w_outgate,
        w_output,
        w_gate,
        w_up,
        w_down,
    )
    return out, state.reshape(memory.shape)


def fits(tokens, memory, w_gate):
    kv_count = lax.axis_size("kv")
    rows, width = tokens.shape
    live_rows = (rows // NEW) * 7 // 4
    groups = -(-live_rows // 16) * 16 // GROUP
    return (
        lax.axis_size("tp") == 2
        and memory.shape[0] == 1
        and memory.shape[1] == 8
        and rows == kv_count * NEW
        and rows % 16 == 0
        and width % TILE == 0
        and kv_count % groups == 0
        and w_gate.shape[1] % (kv_count // groups * TILE) == 0
    )


def layer(*arrays):
    if fits(arrays[0], arrays[2], arrays[15]):
        return fused_device(*arrays)
    return per_device(*arrays)


def solution(mesh):
    placed = (
        P(None, "kv"),
        P(),
        P("kv", "tp", None, None),
        P("kv"),
        P("kv", "tp"),
        P("kv", "tp"),
        P("kv", "tp"),
        P("kv", "tp"),
        P("kv", None),
        P("kv", None),
        P("tp"),
        P("tp"),
        P(),
        P("tp", "kv"),
        P("kv"),
        P("kv", "tp"),
        P("kv", "tp"),
        P("tp", "kv"),
    )
    return jax.shard_map(
        layer,
        mesh=mesh,
        in_specs=placed,
        out_specs=(P(None, "kv"), P("kv", "tp", None, None)),
        check_vma=False,
    )
```

```python
import jax
import jax.numpy as jnp
from jax import lax
from jax.experimental import pallas as pl
from jax.experimental.pallas import tpu as pltpu
from jax.sharding import PartitionSpec as P

D = 4096
DK = 128
DV = 128
NEW = 4


epsilon = 1e-06


def unit_rows(values):
    return values * lax.rsqrt(jnp.sum(values * values, axis=-1, keepdims=True) + epsilon)


def advance(memory, queries, key_rows, value_rows, decays, betas):
    outputs = []
    for step in range(queries.shape[1]):
        memory = jnp.exp(decays[:, step])[:, :, None, None] * memory
        predicted = jnp.einsum(
            "shde,shd->she", memory, key_rows[:, step], precision=lax.Precision.HIGHEST
        )
        correction = betas[:, step][:, :, None] * (value_rows[:, step] - predicted)
        memory = memory + key_rows[:, step][:, :, :, None] * correction[:, :, None, :]
        outputs.append(
            jnp.einsum("shde,shd->she", memory, queries[:, step], precision=lax.Precision.HIGHEST)
        )
    return (memory, jnp.stack(outputs, axis=1))


def per_device(
    tokens,
    lengths,
    memory,
    norm_gain,
    w_query,
    w_key,
    w_value,
    w_outgate,
    w_alpha,
    w_beta,
    decay_log,
    decay_bias,
    head_gain,
    w_output,
    mlp_gain,
    w_gate,
    w_up,
    w_down,
):
    total_rows = tokens.shape[0]
    kv_count = lax.axis_size("kv")
    kv_place = lax.axis_index("kv")
    tp_place = lax.axis_index("tp")
    own_rows = total_rows // kv_count
    seq_dev = memory.shape[0]
    heads_dev = memory.shape[1]
    token_f = tokens.astype(jnp.float32)
    squares = jnp.sum(token_f * token_f, axis=1)
    scaled = (token_f * norm_gain).astype(jnp.bfloat16)
    part_query = jnp.dot(scaled, w_query, preferred_element_type=jnp.float32)
    part_key = jnp.dot(scaled, w_key, preferred_element_type=jnp.float32)
    part_value = jnp.dot(scaled, w_value, preferred_element_type=jnp.float32)
    part_gate = jnp.dot(scaled, w_outgate, preferred_element_type=jnp.float32)
    part_alpha = jnp.dot(scaled, w_alpha, preferred_element_type=jnp.float32)
    part_beta = jnp.dot(scaled, w_beta, preferred_element_type=jnp.float32)
    all_squares = lax.psum(squares, "kv")
    sum_query, sum_key, sum_value, sum_gate, sum_alpha, sum_beta = (
        lax.psum_scatter(part_query, "kv", scatter_dimension=0, tiled=True),
        lax.psum_scatter(part_key, "kv", scatter_dimension=0, tiled=True),
        lax.psum_scatter(part_value, "kv", scatter_dimension=0, tiled=True),
        lax.psum_scatter(part_gate, "kv", scatter_dimension=0, tiled=True),
        lax.psum_scatter(part_alpha, "kv", scatter_dimension=0, tiled=True),
        lax.psum_scatter(part_beta, "kv", scatter_dimension=0, tiled=True),
    )
    own_squares = lax.dynamic_slice_in_dim(all_squares, kv_place * own_rows, own_rows)
    rstd = lax.rsqrt(own_squares / D + epsilon)[:, None]
    queries = (sum_query * rstd).astype(jnp.bfloat16)
    key_rows = (sum_key * rstd).astype(jnp.bfloat16)
    value_rows = (sum_value * rstd).astype(jnp.bfloat16)
    outgate = (sum_gate * rstd).astype(jnp.bfloat16)
    alphas = lax.dynamic_slice_in_dim(sum_alpha * rstd, tp_place * heads_dev, heads_dev, 1)
    beta_pre = lax.dynamic_slice_in_dim(sum_beta * rstd, tp_place * heads_dev, heads_dev, 1)
    own_lengths = lax.dynamic_slice_in_dim(lengths, kv_place * seq_dev, seq_dev)
    live = jnp.arange(NEW, dtype=jnp.int32)[None, :] < own_lengths[:, None]
    query_h = unit_rows(queries.astype(jnp.float32).reshape(seq_dev, NEW, heads_dev, DK)) * DK ** (
        -0.5
    )
    key_h = unit_rows(key_rows.astype(jnp.float32).reshape(seq_dev, NEW, heads_dev, DK))
    value_h = value_rows.astype(jnp.float32).reshape(seq_dev, NEW, heads_dev, DV)
    decays = -jnp.exp(decay_log) * jax.nn.softplus(alphas + decay_bias)
    decays = jnp.where(live[:, :, None], decays.reshape(seq_dev, NEW, heads_dev), 0.0)
    betas = jnp.where(
        live[:, :, None], jax.nn.sigmoid(beta_pre).reshape(seq_dev, NEW, heads_dev), 0.0
    )
    new_memory, attended = advance(memory, query_h, key_h, value_h, decays, betas)
    attended = attended * lax.rsqrt(jnp.mean(attended * attended, axis=-1, keepdims=True) + epsilon)
    gate_h = outgate.astype(jnp.float32).reshape(seq_dev, NEW, heads_dev, DV)
    mixed = (
        (attended * head_gain * jax.nn.silu(gate_h))
        .astype(jnp.bfloat16)
        .reshape(own_rows, heads_dev * DV)
    )
    attn_terms = jnp.dot(
        lax.all_gather(mixed, "kv", axis=0, tiled=True),
        w_output,
        preferred_element_type=jnp.float32,
    )
    attn_total = lax.psum(attn_terms, "tp")
    hidden = (token_f + attn_total).astype(jnp.bfloat16)
    hidden_f = hidden.astype(jnp.float32)
    hidden_squares = jnp.sum(hidden_f * hidden_f, axis=1)
    hscaled = (hidden_f * mlp_gain).astype(jnp.bfloat16)
    all_live = (jnp.arange(NEW, dtype=jnp.int32)[None, :] < lengths[:, None]).reshape(total_rows)
    part_gate_rows = jnp.dot(hscaled, w_gate, preferred_element_type=jnp.float32)
    part_up_rows = jnp.dot(hscaled, w_up, preferred_element_type=jnp.float32)
    gate_rows, up_rows, mlp_squares = lax.psum((part_gate_rows, part_up_rows, hidden_squares), "kv")
    rstd2 = lax.rsqrt(mlp_squares / D + epsilon)[:, None]
    active = (jax.nn.silu(gate_rows * rstd2) * (up_rows * rstd2)).astype(jnp.bfloat16)
    feed_terms = jnp.dot(active, w_down, preferred_element_type=jnp.float32)
    feed_total = lax.psum(feed_terms.astype(jnp.bfloat16), "tp").astype(jnp.float32)
    layer_out = jnp.where(all_live[:, None], hidden_f + feed_total, 0.0).astype(jnp.bfloat16)
    return (layer_out, new_memory)


F32 = jnp.float32
BF16 = jnp.bfloat16
HIGH = lax.Precision.HIGHEST
TILE = 128
GROUP = 8


def iota(shape, axis):
    return lax.broadcasted_iota(jnp.int32, shape, axis)


def dot(a, b, precision=None):
    return jnp.dot(a, b, preferred_element_type=F32, precision=precision)


def fused(
    lens,
    tokens,
    norm_gain,
    decay_log,
    decay_bias,
    head_gain,
    mlp_gain,
    w_alpha,
    w_beta,
    memory,
    w_query,
    w_key,
    w_value,
    w_outgate,
    w_output,
    w_gate,
    w_up,
    w_down,
    out,
    new_memory,
    v_mem,
    v_query,
    v_key,
    v_value,
    v_outgate,
    v_output,
    v_gate,
    v_up,
    v_down,
    proj_send,
    proj_recv,
    proj_part,
    proj_last,
    small_send,
    small_recv,
    rs_buf,
    xs_buf,
    kq_buf,
    r_buf,
    u_buf,
    a_buf,
    ab_buf,
    mix_buf,
    mix_all,
    tp_send,
    tp_recv,
    sq_send,
    sq_recv,
    gu_send,
    gu_recv,
    gu_part,
    gu_last,
    act_all,
    load_sem,
    send_sem,
    recv_sem,
    tp_sem,
):
    kv_count = mix_all.shape[0]
    me = lax.axis_index("kv")
    tp = lax.axis_index("tp")
    rows, width = tokens.shape
    heads = v_mem.shape[0]
    wide = heads * DV
    compact = tp_send.shape[1]
    groups = compact // GROUP
    zones = kv_count // groups
    chunk = gu_send.shape[2]
    total_width = width * kv_count

    barrier = pltpu.get_barrier_semaphore()

    @pl.loop(1, kv_count)
    def _(off):
        pl.semaphore_signal(
            barrier,
            inc=1,
            device_id={"kv": lax.rem(me + off, kv_count)},
            device_id_type=pl.DeviceIdType.MESH,
        )

    pl.semaphore_signal(
        barrier, inc=1, device_id={"tp": 1 - tp}, device_id_type=pl.DeviceIdType.MESH
    )
    pairs = [
        (w_query, v_query),
        (w_key, v_key),
        (w_value, v_value),
        (w_outgate, v_outgate),
        (memory, v_mem),
        (w_output, v_output),
        (w_gate, v_gate),
        (w_up, v_up),
        (w_down, v_down),
    ]
    loads = [pltpu.make_async_copy(a, b, load_sem.at[n]) for n, (a, b) in enumerate(pairs)]
    for load in loads[:4]:
        load.start()

    def remote(src, dst, phase, slot, partner, arrival):
        return pltpu.make_async_remote_copy(
            src_ref=src,
            dst_ref=dst,
            send_sem=send_sem.at[phase, slot],
            recv_sem=recv_sem.at[phase, arrival],
            device_id={"kv": partner},
            device_id_type=pl.DeviceIdType.MESH,
        )

    def tp_swap(phase, value):
        tp_send[phase] = value
        swap = pltpu.make_async_remote_copy(
            src_ref=tp_send.at[phase],
            dst_ref=tp_recv.at[phase],
            send_sem=tp_sem.at[phase, 0],
            recv_sem=tp_sem.at[phase, 1],
            device_id={"tp": 1 - tp},
            device_id_type=pl.DeviceIdType.MESH,
        )
        swap.start()
        swap.wait()
        return value + tp_recv[phase]

    all_rows = kv_count * 4 * NEW
    row = iota((all_rows, rows), 0)
    spread = jnp.where(
        iota((all_rows, rows), 1) == (row >> 4) * NEW + (row & 3), 1.0, 0.0
    ).astype(BF16)
    tok = tokens[...]
    scaled = (tok.astype(F32) * norm_gain[...]).astype(BF16)
    wide_tok = dot(spread, tok)
    wide_scaled = dot(spread, scaled)
    squares = jnp.sum(wide_tok * wide_tok, axis=1, keepdims=True)
    part_of = (iota((all_rows, width), 0) >> 2) & 3
    all_heads = w_alpha.shape[0]
    place = iota((TILE, all_heads), 0)
    head_of = iota((TILE, all_heads), 1)
    w_small = dot(jnp.where(place == head_of, 1.0, 0.0).astype(BF16), w_alpha[...]) + dot(
        jnp.where(place == head_of + all_heads, 1.0, 0.0).astype(BF16), w_beta[...]
    )
    small = lax.dot_general(
        wide_scaled.astype(BF16),
        w_small.astype(BF16),
        (((1,), (1,)), ((), ())),
        preferred_element_type=F32,
    )
    lane = iota((all_rows, TILE), 1)
    small = jnp.where(lane == 2 * all_heads, squares, small)
    small_send[...] = small.reshape(kv_count, 16, TILE)[:, :GROUP, :]
    masked = [jnp.where(part_of == p, wide_scaled, 0.0).astype(BF16) for p in range(4)]
    for load in loads[:4]:
        load.wait()
    for load in loads[4:]:
        load.start()
    half = wide // 2
    for c in range(2):
        cols = slice(c * half, (c + 1) * half)
        acc = dot(masked[0], v_query[:, cols])
        acc = acc + dot(masked[1], v_key[:, cols])
        acc = acc + dot(masked[2], v_value[:, cols])
        acc = acc + dot(masked[3], v_outgate[:, cols])
        proj_send[:, :, cols] = acc.astype(BF16).reshape(kv_count, 16, half)

    pl.semaphore_wait(barrier, kv_count)

    zone_me = me // groups
    group_me = lax.rem(me, groups)
    steps = [*range(1, zones), 0]
    side, odd = zone_me // 2, lax.rem(zone_me, 2)

    def zone_of(step):
        if zones != 4:
            return lax.rem(zone_me + step, zones)
        across = (1 - side) * 2
        return [zone_me, across + 1 - odd, across + odd, side * 2 + 1 - odd][step]

    def peer(g):
        return lax.rem(group_me + g, groups)

    def send_plane(send, recv, phase, zone):
        for g in range(1, groups):
            slab = zone * groups + peer(g)
            remote(
                send.at[slab],
                recv.at[zone * groups + group_me],
                phase,
                slab,
                zone_me * groups + peer(g),
                zone * groups + group_me,
            ).start()

    def sum_plane(send, recv, phase, zone):
        added = send[zone * groups + group_me].astype(F32)
        for g in range(1, groups):
            slab = zone * groups + peer(g)
            remote(send.at[slab], recv.at[slab], phase, slab, me, slab).wait_recv()
            added = added + recv[slab].astype(F32)
        return added

    def reduce_start(send, recv, part, last, phase):
        for step in steps[:-1]:
            zone = zone_of(step)
            part[zone] = sum_plane(send, recv, phase, zone).astype(BF16)
            remote(
                part.at[zone],
                last.at[zone_me],
                phase + 1,
                zone,
                zone * groups + group_me,
                zone_me,
            ).start()
        return sum_plane(send, recv, phase, zone_me)

    def reduce_end(added, part, last, phase):
        for step in steps[:-1][::-1]:
            zone = zone_of(step)
            remote(part.at[zone], last.at[zone], phase + 1, zone, me, zone).wait_recv()
            added = added + last[zone].astype(F32)
        return added

    @pl.loop(1, kv_count)
    def _(off):
        to = lax.rem(me + off, kv_count)
        remote(small_send.at[to], small_recv.at[me], 5, to, to, me).start()

    for step in steps:
        send_plane(proj_send, proj_recv, 0, zone_of(step))

    slots_wide = kv_count * heads * NEW
    shape_a = (1, rows)
    shape_b = (1, slots_wide)
    shape_c = (rows, compact)
    length_a = jnp.zeros(shape_a, jnp.int32)
    start_a = jnp.zeros(shape_a, jnp.int32)
    length_b = jnp.zeros(shape_b, jnp.int32)
    start_b = jnp.zeros(shape_b, jnp.int32)
    length_c = jnp.zeros(shape_c, jnp.int32)
    start_c = jnp.zeros(shape_c, jnp.int32)
    seq_a = iota(shape_a, 1) >> 2
    seq_b = iota(shape_b, 1) >> 5
    seq_c = iota(shape_c, 0) >> 2
    begin = jnp.int32(0)
    for s in range(kv_count):
        length_a = jnp.where(seq_a == s, lens[s], length_a)
        start_a = jnp.where(seq_a == s, begin, start_a)
        length_b = jnp.where(seq_b == s, lens[s], length_b)
        start_b = jnp.where(seq_b == s, begin, start_b)
        length_c = jnp.where(seq_c == s, lens[s], length_c)
        start_c = jnp.where(seq_c == s, begin, start_c)
        begin = begin + lens[s]
    slot_a = iota(shape_a, 1) & 3
    rank_a = jnp.where(slot_a < length_a, start_a + slot_a, -1)
    pack = jnp.where(rank_a == iota((compact, rows), 0), 1.0, 0.0).astype(BF16)
    slot_c = iota(shape_c, 0) & 3
    rank_c = jnp.where(slot_c < length_c, start_c + slot_c, -1)
    unpack = jnp.where(rank_c == iota(shape_c, 1), 1.0, 0.0).astype(BF16)
    slot_b = iota(shape_b, 1) & 3
    head_b = (iota(shape_b, 1) >> 2) & (heads - 1)
    rank_b = jnp.where(slot_b < length_b, head_b * compact + start_b + slot_b, -1)
    collect = jnp.where(rank_b == iota((heads * compact, slots_wide), 0), 1.0, 0.0).astype(BF16)
    tok_packed = dot(pack, tok)

    total = reduce_start(proj_send, proj_recv, proj_part, proj_last, 0)
    small = small_send[me]
    for off in range(1, kv_count):
        src = lax.rem(me + off, kv_count)
        remote(small_send.at[src], small_recv.at[src], 5, src, src, src).wait_recv()
        small = small + small_recv[src]
    small = small[:NEW]
    lane = iota((NEW, TILE), 1)
    mean_sq = jnp.sum(jnp.where(lane == 2 * all_heads, small, 0.0), axis=1, keepdims=True)
    rstd = lax.rsqrt(mean_sq / total_width + epsilon)
    rstd_wide = jnp.broadcast_to(rstd, (NEW, TILE))
    small = small * rstd
    ab_buf[0:4, :] = small
    for p in range(4):
        rs_buf[p * NEW : (p + 1) * NEW, :] = rstd_wide
    eye = iota((heads, heads), 0) == iota((heads, heads), 1)
    rate = jnp.sum(jnp.where(eye, jnp.exp(decay_log[...]), 0.0), axis=1, keepdims=True)
    bias = jnp.sum(jnp.where(eye, decay_bias[...], 0.0), axis=1, keepdims=True)
    pick = iota((heads, TILE), 1) - iota((heads, TILE), 0)
    own_length = jnp.full((heads, 1), lens[me], jnp.int32)
    decay, beta = [], []
    for t in range(NEW):
        line = ab_buf[t : t + 1, :]
        alpha = jnp.sum(jnp.where(pick == tp * heads, line, 0.0), axis=1, keepdims=True)
        write = jnp.sum(
            jnp.where(pick == tp * heads + all_heads, line, 0.0), axis=1, keepdims=True
        )
        x = alpha + bias
        soft = jnp.maximum(x, 0.0) + jnp.log1p(jnp.exp(-jnp.abs(x)))
        live = own_length > t
        decay.append(jnp.exp(jnp.where(live, -rate * soft, 0.0)))
        beta.append(jnp.where(live, jax.nn.sigmoid(write), 0.0))
    total = reduce_end(total, proj_part, proj_last, 0)
    scale = rs_buf[...]
    for h in range(heads):
        piece = total[:, h * DV : (h + 1) * DV] * scale
        xs_buf[h * 16 : (h + 1) * 16, :] = piece.astype(BF16).astype(F32)

    def slot_rows(ref, index, stride):
        return ref[pl.ds(index, heads, stride=stride), :]

    query, key_rows, value, gate = (
        [slot_rows(xs_buf, p * NEW + t, 16) for t in range(NEW)] for p in range(4)
    )
    query = [unit_rows(x) * DK ** (-0.5) for x in query]
    key_rows = [unit_rows(x) for x in key_rows]
    for t in range(NEW):
        kq_buf[pl.ds(t, heads, stride=8), :] = key_rows[t]
        kq_buf[pl.ds(NEW + t, heads, stride=8), :] = query[t]
    loads[4].wait()
    for h in range(heads):
        r_buf[h * 8 : (h + 1) * 8, :] = dot(kq_buf[h * 8 : (h + 1) * 8, :], v_mem[h], HIGH)
    seen_k = [slot_rows(r_buf, t, 8) for t in range(NEW)]
    seen_q = [slot_rows(r_buf, NEW + t, 8) for t in range(NEW)]

    def inner(a, b):
        return jnp.sum(a * b, axis=1, keepdims=True)

    corrections = []
    for t in range(NEW):
        for r in range(t, NEW):
            seen_k[r] = seen_k[r] * decay[t]
            seen_q[r] = seen_q[r] * decay[t]
        fix = beta[t] * (value[t] - seen_k[t])
        corrections.append(fix)
        for r in range(t, NEW):
            if r > t:
                seen_k[r] = seen_k[r] + inner(key_rows[t], key_rows[r]) * fix
            seen_q[r] = seen_q[r] + inner(key_rows[t], query[r]) * fix
    for t in range(NEW):
        o = seen_q[t]
        o = o * lax.rsqrt(jnp.mean(o * o, axis=1, keepdims=True) + epsilon)
        o = o * head_gain[...] * (gate[t] * jax.nn.sigmoid(gate[t]))
        mix_buf[pl.ds(t, heads, stride=NEW), :] = o
    mix_all[me] = mix_buf[...].astype(BF16)

    @pl.loop(1, kv_count)
    def _(off):
        to = lax.rem(me + off, kv_count)
        remote(mix_all.at[me], mix_all.at[me], 2, to, to, me).start()

    u_buf[...] = jnp.zeros_like(u_buf)
    after = jnp.ones((heads, 1), F32)
    for t in range(NEW - 1, -1, -1):
        u_buf[pl.ds(t, heads, stride=8), :] = corrections[t] * after
        after = after * decay[t]
    a_buf[...] = jnp.broadcast_to(after, (heads, TILE))
    for h in range(heads):
        outer = lax.dot_general(
            kq_buf[h * 8 : (h + 1) * 8, :],
            u_buf[h * 8 : (h + 1) * 8, :],
            (((0,), (0,)), ((), ())),
            precision=HIGH,
            preferred_element_type=F32,
        )
        v_mem[h] = v_mem[h] * a_buf[h : h + 1, :] + outer
    store = pltpu.make_async_copy(v_mem, new_memory, load_sem.at[len(pairs)])
    store.start()

    for off in range(1, kv_count):
        src = lax.rem(me + off, kv_count)
        remote(mix_all.at[src], mix_all.at[src], 2, src, src, src).wait_recv()
    gathered = mix_all[...].reshape(slots_wide, DV)
    packed = dot(collect, gathered).astype(BF16)
    loads[5].wait()
    packed = jnp.concatenate(
        [packed[h * compact : (h + 1) * compact, :] for h in range(heads)], axis=1
    )
    attended = tp_swap(0, dot(packed, v_output[...]))
    hidden = (tok_packed + attended).astype(BF16).astype(F32)
    squares = jnp.broadcast_to(
        jnp.sum(hidden * hidden, axis=1, keepdims=True), (compact, TILE)
    )
    sq_send[...] = squares.reshape(groups, GROUP, TILE)

    @pl.loop(1, kv_count)
    def _(off):
        to = lax.rem(me + off, kv_count)
        remote(sq_send.at[lax.rem(to, groups)], sq_recv.at[me], 6, to, to, me).start()

    hscaled = hidden * mlp_gain[...]
    blank = jnp.zeros((GROUP, width), F32)
    gate_rows, up_rows = [], []
    for g in range(groups):
        own = hscaled[g * GROUP : (g + 1) * GROUP, :]
        gate_rows += [own, blank]
        up_rows += [blank, own]
    gate_rows = jnp.concatenate(gate_rows, axis=0).astype(BF16)
    up_rows = jnp.concatenate(up_rows, axis=0).astype(BF16)
    loads[6].wait()
    loads[7].wait()
    for step in steps:
        zone = zone_of(step)
        cols = pl.ds(pl.multiple_of(zone * chunk, TILE), chunk)
        term = dot(gate_rows, v_gate[:, cols]) + dot(up_rows, v_up[:, cols])
        gu_send[pl.ds(zone * groups, groups)] = term.astype(BF16).reshape(
            groups, 2 * GROUP, chunk
        )
        send_plane(gu_send, gu_recv, 3, zone)
    both = reduce_start(gu_send, gu_recv, gu_part, gu_last, 3)
    mean_sq = sq_send[group_me]
    for off in range(1, kv_count):
        src = lax.rem(me + off, kv_count)
        remote(sq_send.at[0], sq_recv.at[src], 6, src, src, src).wait_recv()
        mean_sq = mean_sq + sq_recv[src]
    rstd2 = lax.rsqrt(mean_sq / total_width + epsilon)[:, :1]
    both = reduce_end(both, gu_part, gu_last, 3)
    gated = both[:GROUP] * rstd2
    active = gated * jax.nn.sigmoid(gated) * (both[GROUP:] * rstd2)
    act_all[me] = active.astype(BF16)

    def pass_on(zone, slot, partner):
        block = zone * groups + group_me
        remote(act_all.at[block], act_all.at[block], 7, slot, partner, block).start()

    def arrive(block):
        remote(act_all.at[block], act_all.at[block], 7, block, me, block).wait_recv()

    def forward(zone):
        for g in range(1, groups):
            pass_on(zone, zone * groups + peer(g), zone_me * groups + peer(g))

    for step in steps[:-1]:
        there = zone_of(step) * groups + group_me
        pass_on(zone_me, there, there)
    forward(zone_me)
    near_first = steps[::-1]
    for step in near_first[1:]:
        zone = zone_of(step)
        arrive(zone * groups + group_me)
        forward(zone)
    loads[8].wait()
    feed = jnp.zeros((compact, width), F32)
    for step in near_first:
        zone = zone_of(step)
        for g in range(1, groups):
            arrive(zone * groups + peer(g))
        part = act_all[pl.ds(zone * groups, groups)].astype(F32).reshape(compact, chunk)
        cols = pl.ds(pl.multiple_of(zone * chunk, TILE), chunk)
        feed = feed + dot(part.astype(BF16), v_down[cols, :])
    result = (hidden + tp_swap(1, feed)).astype(BF16)
    out[...] = dot(unpack, result).astype(BF16)

    store.wait()

    @pl.loop(1, kv_count)
    def _(off):
        to = lax.rem(me + off, kv_count)
        remote(mix_all.at[me], mix_all.at[me], 2, to, to, me).wait_send()
        remote(small_send.at[to], small_recv.at[me], 5, to, to, me).wait_send()
        remote(sq_send.at[0], sq_recv.at[me], 6, to, to, me).wait_send()
        remote(act_all.at[me], act_all.at[me], 7, to, to, me).wait_send()

    for step in steps:
        zone = zone_of(step)
        for g in range(1, groups):
            slab = zone * groups + peer(g)
            remote(proj_send.at[slab], proj_recv.at[slab], 0, slab, me, slab).wait_send()
            remote(gu_send.at[slab], gu_recv.at[slab], 3, slab, me, slab).wait_send()
        if step:
            remote(proj_part.at[zone], proj_last.at[zone], 1, zone, me, zone).wait_send()
            remote(gu_part.at[zone], gu_last.at[zone], 4, zone, me, zone).wait_send()


def fused_device(
    tokens,
    lengths,
    memory,
    norm_gain,
    w_query,
    w_key,
    w_value,
    w_outgate,
    w_alpha,
    w_beta,
    decay_log,
    decay_bias,
    head_gain,
    w_output,
    mlp_gain,
    w_gate,
    w_up,
    w_down,
):
    kv_count = lax.axis_size("kv")
    rows, width = tokens.shape
    heads = memory.shape[1]
    live_rows = (rows // NEW) * 7 // 4
    compact = -(-live_rows // 16) * 16
    groups = compact // GROUP
    zones = kv_count // groups
    chunk = w_gate.shape[1] // zones
    wide = heads * DV
    vmem = pl.BlockSpec(memory_space=pltpu.VMEM)
    far = pl.BlockSpec(memory_space=pl.ANY)
    out, state = pl.pallas_call(
        fused,
        out_shape=(
            jax.ShapeDtypeStruct((rows, width), BF16),
            jax.ShapeDtypeStruct(memory.shape[1:], F32),
        ),
        in_specs=[pl.BlockSpec(memory_space=pltpu.SMEM)] + [vmem] * 8 + [far] * 9,
        out_specs=(vmem, far),
        scratch_shapes=[
            pltpu.VMEM(memory.shape[1:], F32),
            pltpu.VMEM(w_query.shape, BF16),
            pltpu.VMEM(w_key.shape, BF16),
            pltpu.VMEM(w_value.shape, BF16),
            pltpu.VMEM(w_outgate.shape, BF16),
            pltpu.VMEM(w_output.shape, BF16),
            pltpu.VMEM(w_gate.shape, BF16),
            pltpu.VMEM(w_up.shape, BF16),
            pltpu.VMEM(w_down.shape, BF16),
            pltpu.VMEM((kv_count, 16, wide), BF16),
            pltpu.VMEM((kv_count, 16, wide), BF16),
            pltpu.VMEM((zones, 16, wide), BF16),
            pltpu.VMEM((zones, 16, wide), BF16),
            pltpu.VMEM((kv_count, GROUP, TILE), F32),
            pltpu.VMEM((kv_count, GROUP, TILE), F32),
            pltpu.VMEM((16, TILE), F32),
            pltpu.VMEM((heads * 16, TILE), F32),
            pltpu.VMEM((heads * 8, TILE), F32),
            pltpu.VMEM((heads * 8, TILE), F32),
            pltpu.VMEM((heads * 8, TILE), F32),
            pltpu.VMEM((heads, TILE), F32),
            pltpu.VMEM((16, TILE), F32),
            pltpu.VMEM((heads * NEW, TILE), F32),
            pltpu.VMEM((kv_count, heads * NEW, TILE), BF16),
            pltpu.VMEM((2, compact, width), F32),
            pltpu.VMEM((2, compact, width), F32),
            pltpu.VMEM((groups, GROUP, TILE), F32),
            pltpu.VMEM((kv_count, GROUP, TILE), F32),
            pltpu.VMEM((kv_count, 2 * GROUP, chunk), BF16),
            pltpu.VMEM((kv_count, 2 * GROUP, chunk), BF16),
            pltpu.VMEM((zones, 2 * GROUP, chunk), BF16),
            pltpu.VMEM((zones, 2 * GROUP, chunk), BF16),
            pltpu.VMEM((kv_count, GROUP, chunk), BF16),
            pltpu.SemaphoreType.DMA((10,)),
            pltpu.SemaphoreType.DMA((8, kv_count)),
            pltpu.SemaphoreType.DMA((8, kv_count)),
            pltpu.SemaphoreType.DMA((2, 2)),
        ],
        compiler_params=pltpu.CompilerParams(
            collective_id=0, has_side_effects=True, vmem_limit_bytes=67043328
        ),
    )(
        lengths,
        tokens,
        norm_gain.reshape(1, -1),
        decay_log.reshape(1, -1),
        decay_bias.reshape(1, -1),
        head_gain.reshape(1, -1),
        mlp_gain.reshape(1, -1),
        w_alpha.T,
        w_beta.T,
        memory.reshape(memory.shape[1:]),
        w_query,
        w_key,
        w_value,
        w_outgate,
        w_output,
        w_gate,
        w_up,
        w_down,
    )
    return out, state.reshape(memory.shape)


def fits(tokens, memory, w_gate):
    kv_count = lax.axis_size("kv")
    rows, width = tokens.shape
    live_rows = (rows // NEW) * 7 // 4
    groups = -(-live_rows // 16) * 16 // GROUP
    return (
        lax.axis_size("tp") == 2
        and memory.shape[0] == 1
        and memory.shape[1] == 8
        and rows == kv_count * NEW
        and rows % 16 == 0
        and width % TILE == 0
        and kv_count % groups == 0
        and w_gate.shape[1] % (kv_count // groups * TILE) == 0
    )


def layer(*arrays):
    if fits(arrays[0], arrays[2], arrays[15]):
        return fused_device(*arrays)
    return per_device(*arrays)


def solution(mesh):
    placed = (
        P(None, "kv"),
        P(),
        P("kv", "tp", None, None),
        P("kv"),
        P("kv", "tp"),
        P("kv", "tp"),
        P("kv", "tp"),
        P("kv", "tp"),
        P("kv", None),
        P("kv", None),
        P("tp"),
        P("tp"),
        P(),
        P("tp", "kv"),
        P("kv"),
        P("kv", "tp"),
        P("kv", "tp"),
        P("tp", "kv"),
    )
    return jax.shard_map(
        layer,
        mesh=mesh,
        in_specs=placed,
        out_specs=(P(None, "kv"), P("kv", "tp", None, None)),
        check_vma=False,
    )
```
